512 devices in a mesh: sp: 64 (over z, y), tp: 8 (over x, core).
Axes of the slice: x: 4, y: 8, z: 8, core: 2. Of those that a mesh axis runs over, the one named last changes fastest.
Arguments:
- tokens: bfloat16 [16384, 2048], P(('sp', 'tp')), may hold values from -6 to 6
- gain: float32 [2048], replicated, may hold values from 0.1 to 1.9
- w_ret_q: bfloat16 [2048, 2048], P(None, 'tp'), may hold values from -0.125 to 0.125
- w_ret_k: bfloat16 [2048, 2048], P(None, 'tp'), may hold values from -0.125 to 0.125
- w_ret_v: bfloat16 [2048, 2048], P(None, 'tp'), may hold values from -0.125 to 0.125
- w_fox_q: bfloat16 [2048, 1024], P(None, 'tp'), may hold values from -0.125 to 0.125
- w_fox_k: bfloat16 [2048, 1024], P(None, 'tp'), may hold values from -0.125 to 0.125
- w_fox_v: bfloat16 [2048, 1024], P(None, 'tp'), may hold values from -0.125 to 0.125
- fox_gates: float32 [16384, 8], P('sp', 'tp'), may hold values from -16384 to 0, as said below
- w_out_ret: bfloat16 [2048, 2048], P('tp', 'sp'), may hold values from -0.109375 to 0.109375
- w_out_fox: bfloat16 [1024, 2048], P('tp', 'sp'), may hold values from -0.109375 to 0.109375
Outputs:
- mixed: bfloat16 [16384, 2048], P(('sp', 'tp'))
The draws below stay inside these ranges and needn't reach their ends.
Inputs may be any that keep to these rules, and one draw needn't show every extreme that they name: `fox_gates`: each head's values never rise along positions.
All inputs are finite; a program needn't handle non-finite values.
Results may differ from the reference program's by a relative error of at most 0.02.
Values may be sent and summed in bfloat16 or wider, within the bound.
No kernel may reach another device: no remote copies, remote signals or barrier semaphores. Data moves between devices by JAX's collectives and lax.ppermute only.
A program may use at most 128 MiB of HBM per device.

```python
import math
import jax
import jax.numpy as jnp
from jax import lax

D = 2048
RET_HEADS = 8
RET_DIM = 256
FORGET_HEADS = 8
FOX_DIM = 128
BLOCK = 128
TOK_DEV = 256
SEQUENCE_TOKENS = 16384
N_TP = 8


def draw_fox_gates(key, part):
    ranking = jax.random.permutation(jax.random.fold_in(key, 11), FORGET_HEADS)
    slow_heads = ranking < FORGET_HEADS // 2
    roughness = jax.random.uniform(jax.random.fold_in(key, 14), (SEQUENCE_TOKENS, FORGET_HEADS), jnp.float32, 0.5, 1.5)
    fast_rate = 1.0 / jax.random.uniform(jax.random.fold_in(key, 12), (FORGET_HEADS,), jnp.float32, 30.0, 50.0)
    slow_rate = jax.random.uniform(jax.random.fold_in(key, 13), (FORGET_HEADS,), jnp.float32, 0.1, 0.4) / SEQUENCE_TOKENS
    base_rate = jnp.where(slow_heads, slow_rate, fast_rate)
    block_count = SEQUENCE_TOKENS // TOK_DEV
    block_factor = jnp.exp(jax.random.uniform(jax.random.fold_in(key, 15), (block_count, FORGET_HEADS), jnp.float32, 0.0, math.log(4.0)))
    block_factor = jnp.repeat(block_factor, TOK_DEV, axis=0)
    forget_strength = base_rate[None, :] * roughness * block_factor
    spike_locations = jax.random.randint(jax.random.fold_in(key, 16), (2, FORGET_HEADS), 0, SEQUENCE_TOKENS)
    token_positions = jnp.arange(SEQUENCE_TOKENS, dtype=jnp.int32)
    spike_mask = jnp.any(token_positions[None, :, None] == spike_locations[:, None, :], axis=0)
    retain_fraction = jax.random.uniform(jax.random.fold_in(key, 17), (SEQUENCE_TOKENS, FORGET_HEADS), jnp.float32, 0.5, 0.8)
    forget_strength = forget_strength + jnp.where(spike_mask, -jnp.log(retain_fraction), 0.0)
    return -jnp.cumsum(forget_strength, axis=0)


def block_scale(key, dims, pieces, smallest, high):
    factor_of, own = 1.0, jax.random.fold_in(key, 6)
    for position, parts in pieces:
        draws = jnp.exp(jax.random.uniform(jax.random.fold_in(own, position), (parts,), jnp.float32, smallest / len(pieces), high / len(pieces)))
        factor_of = factor_of * jnp.repeat(draws, dims[position] // parts).reshape([-1 if axis == position else 1 for axis in range(len(dims))])
    return factor_of


def bell_draw(rng, dims, scale, limit, split=(), kind=jnp.bfloat16):
    result = scale * jax.random.normal(rng, dims, jnp.float32)
    if split:
        result = result * block_scale(rng, dims, split, -0.22, 0.18)
    return jnp.clip(result, -limit, limit).astype(kind)


def setup_inputs(seed: int = 0) -> dict:
    splits = jax.random.split(jax.random.key(seed), 12)
    return {
        "tokens": bell_draw(splits[0], (SEQUENCE_TOKENS, D), 1.0, 6.0, ((0, 512),)),
        "gain": jnp.clip(1.0 + 0.18 * jax.random.normal(splits[1], (D,), jnp.float32), 0.1, 1.9),
        "w_ret_q": bell_draw(splits[2], (D, RET_HEADS * RET_DIM), D ** -0.5, 0.125, ((1, 8),)),
        "w_ret_k": bell_draw(splits[3], (D, RET_HEADS * RET_DIM), D ** -0.5, 0.125, ((1, 8),)),
        "w_ret_v": bell_draw(splits[4], (D, RET_HEADS * RET_DIM), D ** -0.5, 0.125, ((1, 8),)),
        "w_fox_q": bell_draw(splits[5], (D, FORGET_HEADS * FOX_DIM), D ** -0.5, 0.125, ((1, 8),)),
        "w_fox_k": bell_draw(splits[6], (D, FORGET_HEADS * FOX_DIM), D ** -0.5, 0.125, ((1, 8),)),
        "w_fox_v": bell_draw(splits[7], (D, FORGET_HEADS * FOX_DIM), D ** -0.5, 0.125, ((1, 8),)),
        "fox_gates": draw_fox_gates(jax.random.fold_in(splits[11], 71), 0),
        "w_out_ret": bell_draw(splits[9], (RET_HEADS * RET_DIM, D), (RET_HEADS * RET_DIM + FORGET_HEADS * FOX_DIM) ** -0.5, 0.109375, ((0, 8), (1, 64))),
        "w_out_fox": bell_draw(splits[10], (FORGET_HEADS * FOX_DIM, D), (RET_HEADS * RET_DIM + FORGET_HEADS * FOX_DIM) ** -0.5, 0.109375, ((0, 8), (1, 64))),
    }


eps = 1e-06

def to_half(values):
    return lax.optimization_barrier(values.astype(jnp.bfloat16))

def head_norm(values, width):
    rows_here = values.shape[0]
    grouped = values.reshape(rows_here, -1, width)
    scaled = grouped * lax.rsqrt(lax.optimization_barrier(jnp.mean(grouped * grouped, axis=2, keepdims=True)) + eps)
    return scaled.reshape(rows_here, -1).astype(jnp.bfloat16)

def rotate(values, token_positions, width):
    rows_here = values.shape[0]
    half_width = width // 2
    inverse = 10000.0 ** (-jnp.arange(half_width, dtype=jnp.float32) / half_width)
    angles = token_positions.astype(jnp.float32)[:, None] * inverse[None, :]
    cosine = jnp.cos(angles)[:, None, :]
    sine = jnp.sin(angles)[:, None, :]
    grouped = values.astype(jnp.float32).reshape(rows_here, -1, width)
    first_half = grouped[..., :half_width]
    second_half = grouped[..., half_width:]
    turned = jnp.concatenate([first_half * cosine - second_half * sine, first_half * sine + second_half * cosine], axis=-1)
    return turned.reshape(rows_here, -1)

def decay_rates(head_ids, total):
    heads_float = head_ids.astype(jnp.float32)
    middle = RET_HEADS // 2
    fast_rate = 1.0 / (32.0 + 16.0 * heads_float)
    slow_rate = jnp.exp2(-(heads_float - middle)) / total
    return jnp.where(head_ids < middle, fast_rate, slow_rate)

def decay_tables(rates):
    offsets = jnp.arange(BLOCK, dtype=jnp.float32)
    spread = offsets[:, None] - offsets[None, :]
    causal = spread >= 0
    within = jnp.where(causal[None], jnp.exp(-rates[:, None, None] * jnp.where(causal, spread, 0.0)[None]), 0.0)
    query_decay = jnp.exp(-rates[None, :] * (offsets[:, None] + 1.0))
    key_decay = jnp.exp(-rates[None, :] * (BLOCK - 1.0 - offsets[:, None]))
    block_decay = jnp.exp(-rates * BLOCK)
    return (within, query_decay, key_decay, block_decay)

def retention(queries, keys, values, rates):
    heads = RET_HEADS
    within, query_decay, key_decay, block_decay = decay_tables(rates)
    count = queries.shape[0] // BLOCK

    def shaped(array):
        return array.astype(jnp.float32).reshape(count, BLOCK, heads, RET_DIM)

    def step(carry, blocks):
        query_block, key_block, value_block = blocks
        scores = jnp.einsum('thd,shd->hts', query_block, key_block, precision=lax.Precision.HIGHEST) * within
        inner = jnp.einsum('hts,she->the', to_half(scores).astype(jnp.float32), value_block, precision=lax.Precision.HIGHEST)
        cross = jnp.einsum('thd,hde->the', query_block, carry, precision=lax.Precision.HIGHEST) * query_decay[:, :, None]
        scaled = to_half(key_block * key_decay[:, :, None]).astype(jnp.float32)
        new_state = carry * block_decay[:, None, None] + jnp.einsum('shd,she->hde', scaled, value_block, precision=lax.Precision.HIGHEST)
        return (new_state, inner + cross)
    start_state = jnp.zeros((heads, RET_DIM, RET_DIM), jnp.float32)
    _, outputs = lax.scan(step, start_state, (shaped(queries), shaped(keys), shaped(values)))
    return outputs.reshape(count * BLOCK, heads * RET_DIM)

def forgetting(queries, keys, values, gates):
    total = queries.shape[0]
    heads = FORGET_HEADS
    width = math.gcd(total, 512)
    query3 = queries.astype(jnp.float32).reshape(total, heads, FOX_DIM)
    key3 = keys.astype(jnp.float32).reshape(total, heads, FOX_DIM)
    value3 = values.astype(jnp.float32).reshape(total, heads, FOX_DIM)
    key_pos = jnp.arange(total, dtype=jnp.int32)

    def one_block(index):
        begin = (index * width).astype(jnp.int32)
        block = lax.dynamic_slice_in_dim(query3, begin, width, 0)
        query_gates = lax.dynamic_slice_in_dim(gates, begin, width, 0)
        scores = jnp.einsum('qhd,khd->hqk', block, key3, precision=lax.Precision.HIGHEST) * FOX_DIM ** (-0.5)
        scores = scores + query_gates.T[:, :, None] - gates.T[:, None, :]
        query_pos = begin + jnp.arange(width, dtype=jnp.int32)
        allowed = key_pos[None, :] <= query_pos[:, None]
        weights = jnp.exp(jnp.where(allowed[None], scores, -jnp.inf))
        denom = lax.optimization_barrier(jnp.sum(weights, axis=2))
        numer = jnp.einsum('hqk,khd->qhd', to_half(weights).astype(jnp.float32), value3, precision=lax.Precision.HIGHEST)
        return numer / denom.T[:, :, None]
    outputs = lax.map(one_block, jnp.arange(total // width, dtype=jnp.int32))
    return outputs.reshape(total, heads * FOX_DIM)

def reference(tokens, gain, w_ret_q, w_ret_k, w_ret_v, w_fox_q, w_fox_k, w_fox_v, fox_gates, w_out_ret, w_out_fox):
    inputs = tokens.astype(jnp.float32)
    normed = (inputs * lax.rsqrt(lax.optimization_barrier(jnp.mean(inputs * inputs, axis=1, keepdims=True)) + eps) * gain).astype(jnp.bfloat16)
    ret_query = to_half(jnp.dot(normed, w_ret_q, preferred_element_type=jnp.float32))
    ret_key = to_half(jnp.dot(normed, w_ret_k, preferred_element_type=jnp.float32))
    ret_value = to_half(jnp.dot(normed, w_ret_v, preferred_element_type=jnp.float32))
    fox_query = to_half(jnp.dot(normed, w_fox_q, preferred_element_type=jnp.float32))
    fox_key = to_half(jnp.dot(normed, w_fox_k, preferred_element_type=jnp.float32))
    fox_value = to_half(jnp.dot(normed, w_fox_v, preferred_element_type=jnp.float32))
    token_positions = jnp.arange(SEQUENCE_TOKENS, dtype=jnp.int32)
    query_rot = to_half(rotate(ret_query, token_positions, RET_DIM))
    key_rot = to_half(rotate(ret_key, token_positions, RET_DIM) * RET_DIM ** (-0.5))
    rates = decay_rates(jnp.arange(RET_HEADS, dtype=jnp.int32), float(SEQUENCE_TOKENS))
    ret_mixed = head_norm(retention(query_rot, key_rot, ret_value, rates), RET_DIM)
    fox_mixed = head_norm(forgetting(fox_query, fox_key, fox_value, fox_gates), FOX_DIM)
    ret_run = ret_mixed.shape[1] // N_TP
    fox_run = fox_mixed.shape[1] // N_TP

    def group(total, index):
        ret_rows = lax.dynamic_slice_in_dim(ret_mixed, index * ret_run, ret_run, 1)
        ret_weight = lax.dynamic_slice_in_dim(w_out_ret, index * ret_run, ret_run, 0)
        fox_rows = lax.dynamic_slice_in_dim(fox_mixed, index * fox_run, fox_run, 1)
        fox_weight = lax.dynamic_slice_in_dim(w_out_fox, index * fox_run, fox_run, 0)
        partial_sum = jnp.dot(ret_rows, ret_weight, preferred_element_type=jnp.float32) + jnp.dot(fox_rows, fox_weight, preferred_element_type=jnp.float32)
        return (total + to_half(partial_sum).astype(jnp.float32), None)
    summed, _ = lax.scan(group, jnp.zeros((SEQUENCE_TOKENS, D), jnp.float32), jnp.arange(N_TP, dtype=jnp.int32))
    return summed.astype(jnp.bfloat16)
```

```python
import functools
import math

import jax
import jax.numpy as jnp
import numpy as np
from jax import lax
from jax.experimental import pallas as pl
from jax.experimental.pallas import tpu as pltpu
from jax.sharding import Mesh
from jax.sharding import PartitionSpec as P

N = 8
RUN = 256
LANES = 128
RET = 256
FOX = 128
eps = 1e-06
ALL = ("z", "y", "x", "c")
SP = ("z", "y")
TP = ("x", "c")

Q0, QG0, SA0, SB0, W0, R1 = 0, 256, 272, 336, 400, 496
K0, V0, KG0, TA0, TB0, WW0, R2 = 0, 256, 512, 528, 592, 656, 1424
N0, D0, CA0, CB0, R3 = 0, 256, 272, 336, 400

HEADS = np.arange(8, dtype=np.float64)
RATES = np.where(HEADS < 4, 1.0 / (32.0 + 16.0 * HEADS), np.exp2(-(HEADS - 4)) / 16384.0)
RATE_ROWS = np.stack([RATES, np.exp(-RATES * RUN), np.exp(-RATES * RUN * N)]).astype(np.float32)
INVERSE = 10000.0 ** (-np.arange(LANES, dtype=np.float64) / LANES)
ROW_ANGLE = np.arange(RUN, dtype=np.float64)[:, None] * INVERSE
RUN_ANGLE = (RUN * np.arange(64, dtype=np.float64))[:, None] * INVERSE
ROW_TURN = np.stack([np.cos(ROW_ANGLE), np.sin(ROW_ANGLE)]).astype(np.float32)
RUN_TURN = np.stack([np.cos(RUN_ANGLE), np.sin(RUN_ANGLE)]).astype(np.float32)

BF = jnp.bfloat16
F32 = jnp.float32


def device_id(z, y, x, c):
    return ((z * N + y) * 4 + x) * 2 + c


Y_GROUPS = [[[device_id(z, y, x, c) for y in range(N)] for z in range(N) for x in range(4)] for c in (0, 1)]
Z_GROUPS = [[[device_id(z, y, x, c) for z in range(N)] for y in range(N) for x in range(4)] for c in (0, 1)]
GROUPS_A = Y_GROUPS[0] + Z_GROUPS[1]
GROUPS_B = Z_GROUPS[0] + Y_GROUPS[1]


def exchanged(message, groups):
    return lax.all_to_all(message, ALL, 0, 0, axis_index_groups=groups, tiled=True)


def swapped(array):
    return lax.ppermute(array, "c", [(0, 1), (1, 0)])


def places():
    z, y, c = lax.axis_index("z"), lax.axis_index("y"), lax.axis_index("c")
    first = c == 0
    return z * N + y, jnp.where(first, y, z), jnp.where(first, z, y), c


def dot_nt(left, right):
    return lax.dot_general(left, right, (((1,), (1,)), ((), ())), preferred_element_type=F32)


def dot_tn(left, right):
    return lax.dot_general(left, right, (((0,), (0,)), ((), ())), preferred_element_type=F32)


def dot(left, right):
    return jnp.dot(left, right, preferred_element_type=F32)


def project_kernel(
    rates, own, other, gain, wrq, wrk, wrv, wfq, wfk, wfv, gates, wt, row_turn, run_turn,
    m1, states, kvg, qrot, inner, xs,
):
    place, _, _, c = places()
    head = lax.axis_index("x") * 2 + c
    rate = rates[0, head]
    for j in range(4):
        for part, side in ((own, c), (other, 1 - c)):
            x = part[j].astype(F32)
            scaled = x * lax.rsqrt(jnp.mean(x * x, axis=1, keepdims=True) + eps) * gain[...]
            xs[pl.ds(pl.multiple_of(64 * j + 32 * side, 32), 32), :] = scaled.astype(BF)
    x = xs[...]
    cos_run = run_turn[0, pl.ds(place, 1), :]
    sin_run = run_turn[1, pl.ds(place, 1), :]
    cosine = row_turn[0] * cos_run - row_turn[1] * sin_run
    sine = row_turn[1] * cos_run + row_turn[0] * sin_run

    def turned(values, scale):
        first, second = values[:, :LANES], values[:, LANES:]
        return jnp.concatenate(
            [(first * cosine - second * sine) * scale, (first * sine + second * cosine) * scale], axis=1
        )

    rk = turned(dot(x, wrk[...]).astype(BF).astype(F32), RET**-0.5).astype(BF)
    rv = dot(x, wrv[...]).astype(BF)
    row = lax.broadcasted_iota(jnp.int32, (RUN, RET), 0)
    col = lax.broadcasted_iota(jnp.int32, (RUN, RET), 1)
    kd = (rk.astype(F32) * jnp.exp(-rate * (RUN - 1 - row).astype(F32))).astype(BF)
    state = dot_tn(kd, rv).astype(BF)
    for j in range(N):
        for half in range(2):
            piece = state[32 * j : 32 * j + 32, LANES * half : LANES * half + LANES]
            states[j, 32 * half : 32 * half + 32, :] = piece
            m1[j, SA0 + 32 * half : SA0 + 32 * half + 32, :] = piece
            m1[j, SB0 + 32 * half : SB0 + 32 * half + 32, :] = piece
    rq = turned(dot(x, wrq[...]).astype(BF).astype(F32), 1.0).astype(BF)
    qrot[...] = rq
    spread = row - col
    within = jnp.where(spread >= 0, jnp.exp(-rate * jnp.maximum(spread, 0).astype(F32)), 0.0)
    inner[...] = dot((dot_nt(rq, rk) * within).astype(BF), rv)
    fq = dot(x, wfq[...]).astype(BF)
    kvg[K0 : K0 + RUN, :] = dot(x, wfk[...]).astype(BF)
    kvg[V0 : V0 + RUN, :] = dot(x, wfv[...]).astype(BF)
    line = lax.broadcasted_iota(jnp.int32, (16, LANES), 0)
    gate = jnp.where(line < 8, gates[0:1, :], gates[1:2, :]) * (FOX**0.5)
    high = gate.astype(BF).astype(F32)
    middle = (gate - high).astype(BF).astype(F32)
    low = gate - high - middle
    slot = line & 7
    third = jnp.where(slot == 0, high, jnp.where(slot == 1, middle, low))
    of_query = jnp.where(slot < 3, third, jnp.where(slot < 6, 1.0, 0.0)).astype(BF)
    third = jnp.where(slot == 3, high, jnp.where(slot == 4, middle, low))
    of_key = jnp.where(slot < 3, 1.0, jnp.where(slot < 6, -third, 0.0)).astype(BF)
    kvg[KG0 : KG0 + 16, :] = of_key
    for j in range(N):
        m1[j, Q0 : Q0 + RUN, :] = fq
        m1[j, QG0 : QG0 + 16, :] = of_query
        for k in range(3):
            m1[j, W0 + 32 * k : W0 + 32 * k + 32, :] = wt[k]


def totals_kernel(rates, got1, kvg, m2):
    head = lax.axis_index("x") * 2 + lax.axis_index("c")
    sums = []
    for start, which in ((SA0, head), (SB0, head ^ 1)):
        decay = rates[1, which]
        total = got1[0, start : start + 64, :].astype(F32)
        for j in range(1, N):
            total = total * decay + got1[j, start : start + 64, :].astype(F32)
        sums.append(total.astype(BF))
    for j in range(N):
        m2[j, 0 : KG0 + 16, :] = kvg[...]
        m2[j, TA0 : TA0 + 64, :] = sums[0]
        m2[j, TB0 : TB0 + 64, :] = sums[1]
        for k in range(N):
            m2[j, WW0 + 96 * k : WW0 + 96 * k + 96, :] = got1[k, W0 : W0 + 96, :]


def as_columns(rows, eye):
    lines = rows.astype(F32)
    wide = jnp.concatenate([lines[0:8], lines[8:16]], axis=1)
    wide = jnp.concatenate([wide, jnp.zeros((LANES - 8, RUN), F32)], axis=0).astype(BF)
    return dot_nt(eye, wide).astype(BF)


def attention_kernel(rates, got1, got2, m3, keys, values):
    _, a, b, c = places()
    head = lax.axis_index("x") * 2 + c
    row = lax.broadcasted_iota(jnp.int32, (RUN, RUN), 0)
    col = lax.broadcasted_iota(jnp.int32, (RUN, RUN), 1)
    eye = jnp.where(row == col, 1.0, 0.0).astype(BF)
    diagonal = (row == col)[:LANES, :LANES]
    ahead = col - row
    for i in range(N):
        keys[i, :, :LANES] = got2[i, K0 : K0 + RUN, :]
        keys[i, :, LANES:] = as_columns(got2[i, KG0 : KG0 + 16, :], eye)
        values[i, :, :LANES] = got2[i, V0 : V0 + RUN, :]
        values[i, :, LANES:] = jnp.ones((RUN, LANES), BF)

    def one_run(j, carry):
        query = jnp.concatenate(
            [got1[j, Q0 : Q0 + RUN, :], as_columns(got1[j, QG0 : QG0 + 16, :], eye)], axis=1
        )
        of_query = jnp.where(c == 0, b * N + j, j * N + b)
        total = jnp.zeros((RUN, 2 * LANES), F32)
        for i in range(N):
            of_key = jnp.where(c == 0, i * N + a, a * N + i)
            score = dot_nt(query, keys[i]) * (FOX**-0.5 * math.log2(math.e))
            score = jnp.where(ahead <= (of_query - of_key) * RUN, score, -jnp.inf)
            total = total + dot(jnp.exp2(score).astype(BF), values[i])
        m3[j, N0 : N0 + RUN, :] = total[:, :LANES].astype(BF)
        den = [
            jnp.sum(jnp.where(diagonal, total[LANES * h : LANES * h + LANES, LANES:], 0.0), axis=0, keepdims=True)
            for h in range(2)
        ]
        line = lax.broadcasted_iota(jnp.int32, (16, LANES), 0)
        den = jnp.where((line & 1) == 0, den[0], den[1])
        high = den.astype(BF).astype(F32)
        m3[j, D0 : D0 + 16, :] = jnp.where(line < 2, high, jnp.where(line < 4, den - high, 0.0)).astype(BF)
        return carry

    lax.fori_loop(0, N, one_run, 0)
    for own, (sums, slices, carried) in enumerate(((TA0, SA0, CA0), (TB0, SB0, CB0))):
        which = head ^ own
        per_run, per_row = rates[1, which], rates[2, which]
        state = jnp.zeros((64, LANES), F32)
        for k in range(N):
            state = jnp.where(k < b, state * per_row + got2[k, sums : sums + 64, :].astype(F32), state)
        for j in range(N):
            m3[j, carried : carried + 64, :] = state.astype(BF)
            state = state * per_run + got1[j, slices : slices + 64, :].astype(F32)


def output_kernel(rates, got2, got3, sent, qrot, inner, keep, give, weight, mixed, state):
    _, _, _, c = places()
    rate = rates[0, lax.axis_index("x") * 2 + c]
    for i in range(N):
        for k in range(N):
            at = pl.multiple_of(jnp.where(c == 0, i * N + k, k * N + i) * 32, 32)
            for h in range(3):
                start = WW0 + 96 * k + 32 * h
                weight[pl.ds(at, 32), LANES * h : LANES * h + LANES] = got2[i, start : start + 32, :]
    num = got3[0, N0 : N0 + RUN, :].astype(F32)
    den = got3[0, D0 : D0 + 16, :].astype(F32)
    for j in range(1, N):
        num = num + got3[j, N0 : N0 + RUN, :].astype(F32)
        den = den + got3[j, D0 : D0 + 16, :].astype(F32)
    row = lax.broadcasted_iota(jnp.int32, (LANES, LANES), 0)
    col = lax.broadcasted_iota(jnp.int32, (LANES, LANES), 1)
    for h in range(2):
        line = den[h : h + 1, :] + den[h + 2 : h + 3, :]
        column = jnp.sum(jnp.where(row == col, line, 0.0), axis=1, keepdims=True)
        raw = num[LANES * h : LANES * h + LANES] / column
        raw = raw * lax.rsqrt(jnp.mean(raw * raw, axis=1, keepdims=True) + eps)
        mixed[LANES * h : LANES * h + LANES, RET:] = raw.astype(BF)
    for j in range(N):
        for half in range(2):
            start = 32 * half
            piece = jnp.where(
                c == 0, got3[j, CA0 + start : CA0 + start + 32, :].astype(F32), sent[j, start : start + 32, :].astype(F32)
            )
            state[32 * j : 32 * j + 32, LANES * half : LANES * half + LANES] = piece.astype(BF)
    steps = lax.broadcasted_iota(jnp.int32, (RUN, RET), 0)
    raw = inner[...] + dot(qrot[...], state[...]) * jnp.exp(-rate * (steps + 1).astype(F32))
    raw = raw * lax.rsqrt(jnp.mean(raw * raw, axis=1, keepdims=True) + eps)
    mixed[:, :RET] = raw.astype(BF)
    for side, target in ((c, keep), (1 - c, give)):
        rows = jnp.concatenate(
            [mixed[pl.ds(pl.multiple_of(64 * j + 32 * side, 32), 32), :] for j in range(4)], axis=0
        )
        for n in range(4):
            part = dot_nt(rows, weight[512 * n : 512 * n + 512, :])
            for j in range(4):
                target[j, :, 512 * n : 512 * n + 512] = part[32 * j : 32 * j + 32].astype(target.dtype)


def vmem(count):
    return [pl.BlockSpec(memory_space=pltpu.VMEM)] * count


def call(kernel, outs, scratch, args, flops, nbytes, name):
    specs = [pl.BlockSpec(memory_space=pltpu.SMEM)] + vmem(len(args) - 1)
    return pl.pallas_call(
        kernel,
        out_shape=outs,
        in_specs=specs,
        out_specs=vmem(len(outs)),
        scratch_shapes=scratch,
        cost_estimate=pl.CostEstimate(flops=flops, bytes_accessed=nbytes, transcendentals=0),
        name=name,
    )(*args)


def struct(*shape, dtype=BF):
    return jax.ShapeDtypeStruct(shape, dtype)


def per_device(
    tokens, gain, w_ret_q, w_ret_k, w_ret_v, w_fox_q, w_fox_k, w_fox_v, fox_gates, w_out_ret, w_out_fox
):
    rates = jnp.asarray(RATE_ROWS)
    own = lax.all_to_all(jnp.broadcast_to(tokens[None], (4, 32, 2048)), "x", 0, 0, tiled=True)
    other = swapped(own)
    wt = jnp.concatenate([w_out_ret, w_out_fox], axis=0).reshape(3, LANES, 32).transpose(0, 2, 1)
    m1, states, kvg, qrot, inner = call(
        project_kernel,
        [struct(N, R1, LANES), struct(N, 64, LANES), struct(KG0 + 16, LANES), struct(RUN, RET), struct(RUN, RET, dtype=F32)],
        [pltpu.VMEM((RUN, 2048), BF)],
        (
            rates, own, other, gain.reshape(1, 2048), w_ret_q, w_ret_k, w_ret_v, w_fox_q, w_fox_k, w_fox_v,
            fox_gates.reshape(2, LANES), wt, jnp.asarray(ROW_TURN), jnp.asarray(RUN_TURN),
        ),
        1_400_000_000, 8_000_000, "project",
    )
    m1 = lax.dynamic_update_slice(m1, swapped(states), (0, SB0, 0))
    got1 = exchanged(m1, GROUPS_A)
    (m2,) = call(totals_kernel, [struct(N, R2, LANES)], [], (rates, got1, kvg), 1_000_000, 4_000_000, "totals")
    got2 = exchanged(m2, GROUPS_B)
    (m3,) = call(
        attention_kernel,
        [struct(N, R3, LANES)],
        [pltpu.VMEM((N, RUN, 2 * LANES), BF), pltpu.VMEM((N, RUN, 2 * LANES), BF)],
        (rates, got1, got2), 4_300_000_000, 4_000_000, "attention",
    )
    got3 = exchanged(m3, GROUPS_A)
    sent = swapped(got3[:, CB0 : CB0 + 64, :])
    keep, give = call(
        output_kernel,
        [struct(4, 32, 2048, dtype=F32), struct(4, 32, 2048)],
        [pltpu.VMEM((2048, 384), BF), pltpu.VMEM((RUN, 384), BF), pltpu.VMEM((RET, RET), BF)],
        (rates, got2, got3, sent, qrot, inner), 400_000_000, 4_000_000, "output",
    )
    pair = (keep + swapped(give).astype(F32)).astype(BF)
    return jnp.sum(lax.all_to_all(pair, "x", 0, 0, tiled=True).astype(F32), axis=0).astype(BF)


def solution(mesh):
    split = Mesh(mesh.devices.reshape(N, N, 4, 2), ALL)
    return jax.shard_map(
        per_device,
        mesh=split,
        in_specs=(
            P(ALL, None),
            P(),
            P(None, TP),
            P(None, TP),
            P(None, TP),
            P(None, TP),
            P(None, TP),
            P(None, TP),
            P(SP, TP),
            P(TP, SP),
            P(TP, SP),
        ),
        out_specs=P(ALL, None),
        check_vma=False,
    )
```

```python
import functools
import math

import jax
import jax.numpy as jnp
import numpy as np
from jax import lax
from jax.experimental import pallas as pl
from jax.experimental.pallas import tpu as pltpu
from jax.sharding import Mesh
from jax.sharding import PartitionSpec as P

N = 8
RUN = 256
LANES = 128
RET = 256
FOX = 128
eps = 1e-06
ALL = ("z", "y", "x", "c")
SP = ("z", "y")
TP = ("x", "c")

Q0, QG0, SA0, SB0, W0, R1 = 0, 256, 272, 336, 400, 496
K0, V0, KG0, TA0, TB0, WW0, R2 = 0, 256, 512, 528, 592, 656, 1424
N0, D0, CA0, CB0, R3 = 0, 256, 272, 336, 400

HEADS = np.arange(8, dtype=np.float64)
RATES = np.where(HEADS < 4, 1.0 / (32.0 + 16.0 * HEADS), np.exp2(-(HEADS - 4)) / 16384.0)
PER_RUN = np.exp(-RATES * RUN)
PER_ROW = np.exp(-RATES * RUN * N)
INVERSE = 10000.0 ** (-np.arange(LANES, dtype=np.float64) / LANES)
ROW_ANGLE = np.arange(RUN, dtype=np.float64)[:, None] * INVERSE
RUN_ANGLE = (RUN * np.arange(64, dtype=np.float64))[:, None] * INVERSE
ROW_TURN = np.stack([np.cos(ROW_ANGLE), np.sin(ROW_ANGLE)]).astype(np.float32)
RUN_TURN = np.stack([np.cos(RUN_ANGLE), np.sin(RUN_ANGLE)]).astype(np.float32)

BF = jnp.bfloat16
F32 = jnp.float32


def device_id(z, y, x, c):
    return ((z * N + y) * 4 + x) * 2 + c


Y_GROUPS = [[[device_id(z, y, x, c) for y in range(N)] for z in range(N) for x in range(4)] for c in (0, 1)]
Z_GROUPS = [[[device_id(z, y, x, c) for z in range(N)] for y in range(N) for x in range(4)] for c in (0, 1)]
GROUPS_A = Y_GROUPS[0] + Z_GROUPS[1]
GROUPS_B = Z_GROUPS[0] + Y_GROUPS[1]


def exchanged(message, groups):
    return lax.all_to_all(message, ALL, 0, 0, axis_index_groups=groups, tiled=True)


def swapped(array):
    return lax.ppermute(array, "c", [(0, 1), (1, 0)])


def places():
    z, y, c = lax.axis_index("z"), lax.axis_index("y"), lax.axis_index("c")
    first = c == 0
    return z * N + y, jnp.where(first, y, z), jnp.where(first, z, y), c


def of_head(table, head):
    value = jnp.float32(table[0])
    for h in range(1, 8):
        value = jnp.where(head == h, jnp.float32(table[h]), value)
    return value


def dot_nt(left, right):
    return lax.dot_general(left, right, (((1,), (1,)), ((), ())), preferred_element_type=F32)


def dot_tn(left, right):
    return lax.dot_general(left, right, (((0,), (0,)), ((), ())), preferred_element_type=F32)


def dot(left, right):
    return jnp.dot(left, right, preferred_element_type=F32)


def project_kernel(*refs):
    own, other, wt = refs[:3]
    far = refs[3:13]
    m1, states, kvg, qrot, inner, xs = refs[13:19]
    near = refs[19:29]
    sems = refs[29]
    copies = [pltpu.make_async_copy(src, dst, sems.at[k]) for k, (src, dst) in enumerate(zip(far, near))]
    for copy in copies:
        copy.start()
    gain, wrk, wrv, row_turn, run_turn, wrq, wfq, wfk, wfv, gates = near
    place, _, _, c = places()
    rate = of_head(RATES, lax.axis_index("x") * 2 + c)
    copies[0].wait()
    for j in range(4):
        for part, side in ((own, c), (other, 1 - c)):
            x = part[j].astype(F32)
            scaled = x * lax.rsqrt(jnp.mean(x * x, axis=1, keepdims=True) + eps) * gain[...]
            xs[pl.ds(pl.multiple_of(64 * j + 32 * side, 32), 32), :] = scaled.astype(BF)
    x = xs[...]
    for copy in copies[1:5]:
        copy.wait()
    cos_run = run_turn[0, pl.ds(place, 1), :]
    sin_run = run_turn[1, pl.ds(place, 1), :]
    cosine = row_turn[0] * cos_run - row_turn[1] * sin_run
    sine = row_turn[1] * cos_run + row_turn[0] * sin_run

    def turned(values, scale):
        first, second = values[:, :LANES], values[:, LANES:]
        return jnp.concatenate(
            [(first * cosine - second * sine) * scale, (first * sine + second * cosine) * scale], axis=1
        )

    rk = turned(dot(x, wrk[...]).astype(BF).astype(F32), RET**-0.5).astype(BF)
    rv = dot(x, wrv[...]).astype(BF)
    row = lax.broadcasted_iota(jnp.int32, (RUN, RET), 0)
    col = lax.broadcasted_iota(jnp.int32, (RUN, RET), 1)
    kd = (rk.astype(F32) * jnp.exp(-rate * (RUN - 1 - row).astype(F32))).astype(BF)
    state = dot_tn(kd, rv).astype(BF)
    for j in range(N):
        for half in range(2):
            piece = state[32 * j : 32 * j + 32, LANES * half : LANES * half + LANES]
            states[j, 32 * half : 32 * half + 32, :] = piece
            m1[j, SA0 + 32 * half : SA0 + 32 * half + 32, :] = piece
            m1[j, SB0 + 32 * half : SB0 + 32 * half + 32, :] = piece
    for copy in copies[5:]:
        copy.wait()
    rq = turned(dot(x, wrq[...]).astype(BF).astype(F32), 1.0).astype(BF)
    qrot[...] = rq
    spread = row - col
    within = jnp.where(spread >= 0, jnp.exp(-rate * jnp.maximum(spread, 0).astype(F32)), 0.0)
    inner[...] = dot((dot_nt(rq, rk) * within).astype(BF), rv)
    fq = dot(x, wfq[...]).astype(BF)
    kvg[K0 : K0 + RUN, :] = dot(x, wfk[...]).astype(BF)
    kvg[V0 : V0 + RUN, :] = dot(x, wfv[...]).astype(BF)
    line = lax.broadcasted_iota(jnp.int32, (16, LANES), 0)
    gate = jnp.where(line < 8, gates[0:1, :], gates[1:2, :]) * (FOX**0.5)
    high = gate.astype(BF).astype(F32)
    middle = (gate - high).astype(BF).astype(F32)
    low = gate - high - middle
    slot = line & 7
    third = jnp.where(slot == 0, high, jnp.where(slot == 1, middle, low))
    of_query = jnp.where(slot < 3, third, jnp.where(slot < 6, 1.0, 0.0)).astype(BF)
    third = jnp.where(slot == 3, high, jnp.where(slot == 4, middle, low))
    of_key = jnp.where(slot < 3, 1.0, jnp.where(slot < 6, -third, 0.0)).astype(BF)
    kvg[KG0 : KG0 + 16, :] = of_key
    for j in range(N):
        m1[j, Q0 : Q0 + RUN, :] = fq
        m1[j, QG0 : QG0 + 16, :] = of_query
        for k in range(3):
            m1[j, W0 + 32 * k : W0 + 32 * k + 32, :] = wt[k]


def totals_kernel(got1, kvg, m2):
    head = lax.axis_index("x") * 2 + lax.axis_index("c")
    sums = []
    for start, which in ((SA0, head), (SB0, head ^ 1)):
        decay = of_head(PER_RUN, which)
        total = got1[0, start : start + 64, :].astype(F32)
        for j in range(1, N):
            total = total * decay + got1[j, start : start + 64, :].astype(F32)
        sums.append(total.astype(BF))
    for j in range(N):
        m2[j, 0 : KG0 + 16, :] = kvg[...]
        m2[j, TA0 : TA0 + 64, :] = sums[0]
        m2[j, TB0 : TB0 + 64, :] = sums[1]
        for k in range(N):
            m2[j, WW0 + 96 * k : WW0 + 96 * k + 96, :] = got1[k, W0 : W0 + 96, :]


def as_columns(rows, eye):
    lines = rows.astype(F32)
    wide = jnp.concatenate([lines[0:8], lines[8:16]], axis=1)
    wide = jnp.concatenate([wide, jnp.zeros((LANES - 8, RUN), F32)], axis=0).astype(BF)
    return dot_nt(eye, wide).astype(BF)


def attention_kernel(got1, got2, m3, keys, values):
    _, a, b, c = places()
    head = lax.axis_index("x") * 2 + c
    row = lax.broadcasted_iota(jnp.int32, (RUN, RUN), 0)
    col = lax.broadcasted_iota(jnp.int32, (RUN, RUN), 1)
    eye = jnp.where(row == col, 1.0, 0.0).astype(BF)
    diagonal = (row == col)[:LANES, :LANES]
    ahead = col - row
    for i in range(N):
        keys[i, :, :LANES] = got2[i, K0 : K0 + RUN, :]
        keys[i, :, LANES:] = as_columns(got2[i, KG0 : KG0 + 16, :], eye)
        values[i, :, :LANES] = got2[i, V0 : V0 + RUN, :]
        values[i, :, LANES:] = jnp.ones((RUN, LANES), BF)

    def one_run(j, carry):
        query = jnp.concatenate(
            [got1[j, Q0 : Q0 + RUN, :], as_columns(got1[j, QG0 : QG0 + 16, :], eye)], axis=1
        )
        of_query = jnp.where(c == 0, b * N + j, j * N + b)
        total = jnp.zeros((RUN, 2 * LANES), F32)
        for i in range(N):
            of_key = jnp.where(c == 0, i * N + a, a * N + i)
            score = dot_nt(query, keys[i]) * (FOX**-0.5 * math.log2(math.e))
            score = jnp.where(ahead <= (of_query - of_key) * RUN, score, -jnp.inf)
            total = total + dot(jnp.exp2(score).astype(BF), values[i])
        m3[j, N0 : N0 + RUN, :] = total[:, :LANES].astype(BF)
        den = [
            jnp.sum(jnp.where(diagonal, total[LANES * h : LANES * h + LANES, LANES:], 0.0), axis=0, keepdims=True)
            for h in range(2)
        ]
        line = lax.broadcasted_iota(jnp.int32, (16, LANES), 0)
        den = jnp.where((line & 1) == 0, den[0], den[1])
        high = den.astype(BF).astype(F32)
        m3[j, D0 : D0 + 16, :] = jnp.where(line < 2, high, jnp.where(line < 4, den - high, 0.0)).astype(BF)
        return carry

    lax.fori_loop(0, N, one_run, 0)
    for own, (sums, slices, carried) in enumerate(((TA0, SA0, CA0), (TB0, SB0, CB0))):
        which = head ^ own
        per_run, per_row = of_head(PER_RUN, which), of_head(PER_ROW, which)
        state = jnp.zeros((64, LANES), F32)
        for k in range(N):
            state = jnp.where(k < b, state * per_row + got2[k, sums : sums + 64, :].astype(F32), state)
        for j in range(N):
            m3[j, carried : carried + 64, :] = state.astype(BF)
            state = state * per_run + got1[j, slices : slices + 64, :].astype(F32)


def output_kernel(got2, got3, sent, qrot, inner, keep, give, weight, mixed, state):
    _, _, _, c = places()
    rate = of_head(RATES, lax.axis_index("x") * 2 + c)
    for i in range(N):
        for k in range(N):
            at = pl.multiple_of(jnp.where(c == 0, i * N + k, k * N + i) * 32, 32)
            for h in range(3):
                start = WW0 + 96 * k + 32 * h
                weight[pl.ds(at, 32), LANES * h : LANES * h + LANES] = got2[i, start : start + 32, :]
    num = got3[0, N0 : N0 + RUN, :].astype(F32)
    den = got3[0, D0 : D0 + 16, :].astype(F32)
    for j in range(1, N):
        num = num + got3[j, N0 : N0 + RUN, :].astype(F32)
        den = den + got3[j, D0 : D0 + 16, :].astype(F32)
    row = lax.broadcasted_iota(jnp.int32, (LANES, LANES), 0)
    col = lax.broadcasted_iota(jnp.int32, (LANES, LANES), 1)
    for h in range(2):
        line = den[h : h + 1, :] + den[h + 2 : h + 3, :]
        column = jnp.sum(jnp.where(row == col, line, 0.0), axis=1, keepdims=True)
        raw = num[LANES * h : LANES * h + LANES] / column
        raw = raw * lax.rsqrt(jnp.mean(raw * raw, axis=1, keepdims=True) + eps)
        mixed[LANES * h : LANES * h + LANES, RET:] = raw.astype(BF)
    for j in range(N):
        for half in range(2):
            start = 32 * half
            piece = jnp.where(
                c == 0, got3[j, CA0 + start : CA0 + start + 32, :].astype(F32), sent[j, start : start + 32, :].astype(F32)
            )
            state[32 * j : 32 * j + 32, LANES * half : LANES * half + LANES] = piece.astype(BF)
    steps = lax.broadcasted_iota(jnp.int32, (RUN, RET), 0)
    raw = inner[...] + dot(qrot[...], state[...]) * jnp.exp(-rate * (steps + 1).astype(F32))
    raw = raw * lax.rsqrt(jnp.mean(raw * raw, axis=1, keepdims=True) + eps)
    mixed[:, :RET] = raw.astype(BF)
    for side, target in ((c, keep), (1 - c, give)):
        rows = jnp.concatenate(
            [mixed[pl.ds(pl.multiple_of(64 * j + 32 * side, 32), 32), :] for j in range(4)], axis=0
        )
        for n in range(4):
            part = dot_nt(rows, weight[512 * n : 512 * n + 512, :])
            for j in range(4):
                target[j, :, 512 * n : 512 * n + 512] = part[32 * j : 32 * j + 32].astype(target.dtype)


def vmem(count):
    return [pl.BlockSpec(memory_space=pltpu.VMEM)] * count


def call(kernel, outs, scratch, args, flops, nbytes, name, limit, far=()):
    specs = vmem(len(args)) + [pl.BlockSpec(memory_space=pltpu.HBM)] * len(far)
    return pl.pallas_call(
        kernel,
        out_shape=outs,
        in_specs=specs,
        out_specs=vmem(len(outs)),
        scratch_shapes=scratch,
        cost_estimate=pl.CostEstimate(flops=flops, bytes_accessed=nbytes, transcendentals=0),
        compiler_params=pltpu.CompilerParams(vmem_limit_bytes=limit << 20),
        name=name,
    )(*args, *far)


def struct(*shape, dtype=BF):
    return jax.ShapeDtypeStruct(shape, dtype)


def per_device(
    tokens, gain, w_ret_q, w_ret_k, w_ret_v, w_fox_q, w_fox_k, w_fox_v, fox_gates, w_out_ret, w_out_fox
):
    own = lax.all_to_all(jnp.broadcast_to(tokens[None], (4, 32, 2048)), "x", 0, 0, tiled=True)
    other = swapped(own)
    wt = jnp.concatenate([w_out_ret, w_out_fox], axis=0).reshape(3, LANES, 32).transpose(0, 2, 1)
    far = (
        gain.reshape(1, 2048), w_ret_k, w_ret_v, jnp.asarray(ROW_TURN), jnp.asarray(RUN_TURN),
        w_ret_q, w_fox_q, w_fox_k, w_fox_v, fox_gates.reshape(2, LANES),
    )
    m1, states, kvg, qrot, inner = call(
        project_kernel,
        [struct(N, R1, LANES), struct(N, 64, LANES), struct(KG0 + 16, LANES), struct(RUN, RET), struct(RUN, RET, dtype=F32)],
        [pltpu.VMEM((RUN, 2048), BF)] + [pltpu.VMEM(a.shape, a.dtype) for a in far] + [pltpu.SemaphoreType.DMA((len(far),))],
        (own, other, wt), 1_400_000_000, 8_000_000, "project", 60, far,
    )
    m1 = lax.dynamic_update_slice(m1, swapped(states), (0, SB0, 0))
    got1 = exchanged(m1, GROUPS_A)
    (m2,) = call(totals_kernel, [struct(N, R2, LANES)], [], (got1, kvg), 1_000_000, 4_000_000, "totals", 16)
    got2 = exchanged(m2, GROUPS_B)
    (m3,) = call(
        attention_kernel,
        [struct(N, R3, LANES)],
        [pltpu.VMEM((N, RUN, 2 * LANES), BF), pltpu.VMEM((N, RUN, 2 * LANES), BF)],
        (got1, got2), 4_300_000_000, 4_000_000, "attention", 24,
    )
    got3 = exchanged(m3, GROUPS_A)
    sent = swapped(got3[:, CB0 : CB0 + 64, :])
    keep, give = call(
        output_kernel,
        [struct(4, 32, 2048, dtype=F32), struct(4, 32, 2048)],
        [pltpu.VMEM((2048, 384), BF), pltpu.VMEM((RUN, 384), BF), pltpu.VMEM((RET, RET), BF)],
        (got2, got3, sent, qrot, inner), 400_000_000, 4_000_000, "output", 20,
    )
    pair = (keep + swapped(give).astype(F32)).astype(BF)
    return jnp.sum(lax.all_to_all(pair, "x", 0, 0, tiled=True).astype(F32), axis=0).astype(BF)


def solution(mesh):
    split = Mesh(mesh.devices.reshape(N, N, 4, 2), ALL)
    return jax.shard_map(
        per_device,
        mesh=split,
        in_specs=(
            P(ALL, None),
            P(),
            P(None, TP),
            P(None, TP),
            P(None, TP),
            P(None, TP),
            P(None, TP),
            P(None, TP),
            P(SP, TP),
            P(TP, SP),
            P(TP, SP),
        ),
        out_specs=P(ALL, None),
        check_vma=False,
    )
```

```python
import functools
import math

import jax
import jax.numpy as jnp
import numpy as np
from jax import lax
from jax.experimental import pallas as pl
from jax.experimental.pallas import tpu as pltpu
from jax.sharding import Mesh
from jax.sharding import PartitionSpec as P

N = 8
RUN = 256
LANES = 128
RET = 256
FOX = 128
eps = 1e-06
ALL = ("z", "y", "x", "c")
SP = ("z", "y")
TP = ("x", "c")

Q0, QG0, SA0, SB0, W0, R1 = 0, 256, 272, 336, 400, 496
K0, V0, KG0, TA0, TB0, WW0, R2 = 0, 256, 512, 528, 592, 656, 1424
N0, D0, CA0, CB0, R3 = 0, 256, 272, 336, 400

HEADS = np.arange(8, dtype=np.float64)
RATES = np.where(HEADS < 4, 1.0 / (32.0 + 16.0 * HEADS), np.exp2(-(HEADS - 4)) / 16384.0)
PER_RUN = np.exp(-RATES * RUN)
PER_ROW = np.exp(-RATES * RUN * N)
INVERSE = 10000.0 ** (-np.arange(LANES, dtype=np.float64) / LANES)
ROW_ANGLE = np.arange(RUN, dtype=np.float64)[:, None] * INVERSE
RUN_ANGLE = (RUN * np.arange(64, dtype=np.float64))[:, None] * INVERSE
ROW_TURN = np.stack([np.cos(ROW_ANGLE), np.sin(ROW_ANGLE)]).astype(np.float32)
RUN_TURN = np.stack([np.cos(RUN_ANGLE), np.sin(RUN_ANGLE)]).astype(np.float32)

BF = jnp.bfloat16
F32 = jnp.float32


def device_id(z, y, x, c):
    return ((z * N + y) * 4 + x) * 2 + c


Y_GROUPS = [[[device_id(z, y, x, c) for y in range(N)] for z in range(N) for x in range(4)] for c in (0, 1)]
Z_GROUPS = [[[device_id(z, y, x, c) for z in range(N)] for y in range(N) for x in range(4)] for c in (0, 1)]
GROUPS_A = Y_GROUPS[0] + Z_GROUPS[1]
GROUPS_B = Z_GROUPS[0] + Y_GROUPS[1]


def exchanged(message, groups):
    return lax.all_to_all(message, ALL, 0, 0, axis_index_groups=groups, tiled=True)


def swapped(array):
    return lax.ppermute(array, "c", [(0, 1), (1, 0)])


def places():
    z, y, c = lax.axis_index("z"), lax.axis_index("y"), lax.axis_index("c")
    first = c == 0
    return z * N + y, jnp.where(first, y, z), jnp.where(first, z, y), c


def of_head(table, head):
    value = jnp.float32(table[0])
    for h in range(1, 8):
        value = jnp.where(head == h, jnp.float32(table[h]), value)
    return value


def dot_nt(left, right):
    return lax.dot_general(left, right, (((1,), (1,)), ((), ())), preferred_element_type=F32)


def dot_tn(left, right):
    return lax.dot_general(left, right, (((0,), (0,)), ((), ())), preferred_element_type=F32)


def dot(left, right):
    return jnp.dot(left, right, preferred_element_type=F32)


def project_kernel(*refs):
    own, other, wt = refs[:3]
    far = refs[3:13]
    m1, states, kvg, qrot, inner, xs = refs[13:19]
    near = refs[19:29]
    sems = refs[29]
    copies = [pltpu.make_async_copy(src, dst, sems.at[k]) for k, (src, dst) in enumerate(zip(far, near))]
    for copy in copies:
        copy.start()
    gain, wrk, wrv, row_turn, run_turn, wrq, wfq, wfk, wfv, gates = near
    place, _, _, c = places()
    rate = of_head(RATES, lax.axis_index("x") * 2 + c)
    copies[0].wait()
    for j in range(4):
        for part, side in ((own, c), (other, 1 - c)):
            x = part[j].astype(F32)
            scaled = x * lax.rsqrt(jnp.mean(x * x, axis=1, keepdims=True) + eps) * gain[...]
            xs[pl.ds(pl.multiple_of(64 * j + 32 * side, 32), 32), :] = scaled.astype(BF)
    x = xs[...]
    for copy in copies[1:5]:
        copy.wait()
    cos_run = run_turn[0, pl.ds(place, 1), :]
    sin_run = run_turn[1, pl.ds(place, 1), :]
    cosine = row_turn[0] * cos_run - row_turn[1] * sin_run
    sine = row_turn[1] * cos_run + row_turn[0] * sin_run

    def turned(values, scale):
        first, second = values[:, :LANES], values[:, LANES:]
        return jnp.concatenate(
            [(first * cosine - second * sine) * scale, (first * sine + second * cosine) * scale], axis=1
        )

    rk = turned(dot(x, wrk[...]).astype(BF).astype(F32), RET**-0.5).astype(BF)
    rv = dot(x, wrv[...]).astype(BF)
    row = lax.broadcasted_iota(jnp.int32, (RUN, RET), 0)
    col = lax.broadcasted_iota(jnp.int32, (RUN, RET), 1)
    kd = (rk.astype(F32) * jnp.exp(-rate * (RUN - 1 - row).astype(F32))).astype(BF)
    state = dot_tn(kd, rv).astype(BF)
    for j in range(N):
        for half in range(2):
            piece = state[32 * j : 32 * j + 32, LANES * half : LANES * half + LANES]
            states[j, 32 * half : 32 * half + 32, :] = piece
            m1[j, SA0 + 32 * half : SA0 + 32 * half + 32, :] = piece
            m1[j, SB0 + 32 * half : SB0 + 32 * half + 32, :] = piece
    for copy in copies[5:]:
        copy.wait()
    rq = turned(dot(x, wrq[...]).astype(BF).astype(F32), 1.0).astype(BF)
    qrot[...] = rq
    spread = row - col
    within = jnp.where(spread >= 0, jnp.exp(-rate * jnp.maximum(spread, 0).astype(F32)), 0.0)
    inner[...] = dot((dot_nt(rq, rk) * within).astype(BF), rv)
    fq = dot(x, wfq[...]).astype(BF)
    kvg[K0 : K0 + RUN, :] = dot(x, wfk[...]).astype(BF)
    kvg[V0 : V0 + RUN, :] = dot(x, wfv[...]).astype(BF)
    line = lax.broadcasted_iota(jnp.int32, (16, LANES), 0)
    gate = jnp.where(line < 8, gates[0:1, :], gates[1:2, :]) * (FOX**0.5)
    high = gate.astype(BF).astype(F32)
    middle = (gate - high).astype(BF).astype(F32)
    low = gate - high - middle
    slot = line & 7
    third = jnp.where(slot == 0, high, jnp.where(slot == 1, middle, low))
    of_query = jnp.where(slot < 3, third, jnp.where(slot < 6, 1.0, 0.0)).astype(BF)
    third = jnp.where(slot == 3, high, jnp.where(slot == 4, middle, low))
    of_key = jnp.where(slot < 3, 1.0, jnp.where(slot < 6, -third, 0.0)).astype(BF)
    kvg[KG0 : KG0 + 16, :] = of_key
    for j in range(N):
        m1[j, Q0 : Q0 + RUN, :] = fq
        m1[j, QG0 : QG0 + 16, :] = of_query
        for k in range(3):
            m1[j, W0 + 32 * k : W0 + 32 * k + 32, :] = wt[k]


def totals_kernel(got1, kvg, m2):
    head = lax.axis_index("x") * 2 + lax.axis_index("c")
    sums = []
    for start, which in ((SA0, head), (SB0, head ^ 1)):
        decay = of_head(PER_RUN, which)
        total = got1[0, start : start + 64, :].astype(F32)
        for j in range(1, N):
            total = total * decay + got1[j, start : start + 64, :].astype(F32)
        sums.append(total.astype(BF))
    for j in range(N):
        m2[j, 0 : KG0 + 16, :] = kvg[...]
        m2[j, TA0 : TA0 + 64, :] = sums[0]
        m2[j, TB0 : TB0 + 64, :] = sums[1]
        for k in range(N):
            m2[j, WW0 + 96 * k : WW0 + 96 * k + 96, :] = got1[k, W0 : W0 + 96, :]


def as_columns(rows, eye):
    lines = rows.astype(F32)
    wide = jnp.concatenate([lines[0:8], lines[8:16]], axis=1)
    wide = jnp.concatenate([wide, jnp.zeros((LANES - 8, RUN), F32)], axis=0).astype(BF)
    return dot_nt(eye, wide).astype(BF)


def attention_kernel(got1, got2, m3, keys, values):
    _, a, b, c = places()
    head = lax.axis_index("x") * 2 + c
    row = lax.broadcasted_iota(jnp.int32, (RUN, RUN), 0)
    col = lax.broadcasted_iota(jnp.int32, (RUN, RUN), 1)
    eye = jnp.where(row == col, 1.0, 0.0).astype(BF)
    diagonal = (row == col)[:LANES, :LANES]
    ahead = col - row
    for i in range(N):
        keys[i, :, :LANES] = got2[i, K0 : K0 + RUN, :]
        keys[i, :, LANES:] = as_columns(got2[i, KG0 : KG0 + 16, :], eye)
        values[i, :, :LANES] = got2[i, V0 : V0 + RUN, :]
        values[i, :, LANES:] = jnp.ones((RUN, LANES), BF)

    def one_run(j, carry):
        query = jnp.concatenate(
            [got1[j, Q0 : Q0 + RUN, :], as_columns(got1[j, QG0 : QG0 + 16, :], eye)], axis=1
        )
        of_query = jnp.where(c == 0, b * N + j, j * N + b)
        weights = []
        for i in range(N):
            of_key = jnp.where(c == 0, i * N + a, a * N + i)
            score = dot_nt(query, keys[i]) * (FOX**-0.5 * math.log2(math.e))
            score = jnp.where(ahead <= (of_query - of_key) * RUN, score, -jnp.inf)
            weights.append(jnp.exp2(score).astype(BF))
        total = dot(jnp.concatenate(weights, axis=1), values[...].reshape(N * RUN, 2 * LANES))
        m3[j, N0 : N0 + RUN, :] = total[:, :LANES].astype(BF)
        den = [
            jnp.sum(jnp.where(diagonal, total[LANES * h : LANES * h + LANES, LANES:], 0.0), axis=0, keepdims=True)
            for h in range(2)
        ]
        line = lax.broadcasted_iota(jnp.int32, (16, LANES), 0)
        den = jnp.where((line & 1) == 0, den[0], den[1])
        high = den.astype(BF).astype(F32)
        m3[j, D0 : D0 + 16, :] = jnp.where(line < 2, high, jnp.where(line < 4, den - high, 0.0)).astype(BF)
        return carry

    lax.fori_loop(0, N, one_run, 0, unroll=4)
    for own, (sums, slices, carried) in enumerate(((TA0, SA0, CA0), (TB0, SB0, CB0))):
        which = head ^ own
        per_run, per_row = of_head(PER_RUN, which), of_head(PER_ROW, which)
        state = jnp.zeros((64, LANES), F32)
        for k in range(N):
            state = jnp.where(k < b, state * per_row + got2[k, sums : sums + 64, :].astype(F32), state)
        for j in range(N):
            m3[j, carried : carried + 64, :] = state.astype(BF)
            state = state * per_run + got1[j, slices : slices + 64, :].astype(F32)


def output_kernel(got2, got3, sent, qrot, inner, keep, give, weight, mixed, state):
    _, _, _, c = places()
    rate = of_head(RATES, lax.axis_index("x") * 2 + c)
    for i in range(N):
        for k in range(N):
            at = pl.multiple_of(jnp.where(c == 0, i * N + k, k * N + i) * 32, 32)
            for h in range(3):
                start = WW0 + 96 * k + 32 * h
                weight[pl.ds(at, 32), LANES * h : LANES * h + LANES] = got2[i, start : start + 32, :]
    num = got3[0, N0 : N0 + RUN, :].astype(F32)
    den = got3[0, D0 : D0 + 16, :].astype(F32)
    for j in range(1, N):
        num = num + got3[j, N0 : N0 + RUN, :].astype(F32)
        den = den + got3[j, D0 : D0 + 16, :].astype(F32)
    row = lax.broadcasted_iota(jnp.int32, (LANES, LANES), 0)
    col = lax.broadcasted_iota(jnp.int32, (LANES, LANES), 1)
    for h in range(2):
        line = den[h : h + 1, :] + den[h + 2 : h + 3, :]
        column = jnp.sum(jnp.where(row == col, line, 0.0), axis=1, keepdims=True)
        raw = num[LANES * h : LANES * h + LANES] / column
        raw = raw * lax.rsqrt(jnp.mean(raw * raw, axis=1, keepdims=True) + eps)
        mixed[LANES * h : LANES * h + LANES, RET:] = raw.astype(BF)
    for j in range(N):
        for half in range(2):
            start = 32 * half
            piece = jnp.where(
                c == 0, got3[j, CA0 + start : CA0 + start + 32, :].astype(F32), sent[j, start : start + 32, :].astype(F32)
            )
            state[32 * j : 32 * j + 32, LANES * half : LANES * half + LANES] = piece.astype(BF)
    steps = lax.broadcasted_iota(jnp.int32, (RUN, RET), 0)
    raw = inner[...] + dot(qrot[...], state[...]) * jnp.exp(-rate * (steps + 1).astype(F32))
    raw = raw * lax.rsqrt(jnp.mean(raw * raw, axis=1, keepdims=True) + eps)
    mixed[:, :RET] = raw.astype(BF)
    for side, target in ((c, keep), (1 - c, give)):
        rows = jnp.concatenate(
            [mixed[pl.ds(pl.multiple_of(64 * j + 32 * side, 32), 32), :] for j in range(4)], axis=0
        )
        for n in range(4):
            part = dot_nt(rows, weight[512 * n : 512 * n + 512, :])
            for j in range(4):
                target[j, :, 512 * n : 512 * n + 512] = part[32 * j : 32 * j + 32].astype(target.dtype)


def vmem(count):
    return [pl.BlockSpec(memory_space=pltpu.VMEM)] * count


def call(kernel, outs, scratch, args, flops, nbytes, name, limit, far=()):
    specs = vmem(len(args)) + [pl.BlockSpec(memory_space=pltpu.HBM)] * len(far)
    return pl.pallas_call(
        kernel,
        out_shape=outs,
        in_specs=specs,
        out_specs=vmem(len(outs)),
        scratch_shapes=scratch,
        cost_estimate=pl.CostEstimate(flops=flops, bytes_accessed=nbytes, transcendentals=0),
        compiler_params=pltpu.CompilerParams(vmem_limit_bytes=limit << 20),
        name=name,
    )(*args, *far)


def struct(*shape, dtype=BF):
    return jax.ShapeDtypeStruct(shape, dtype)


def per_device(
    tokens, gain, w_ret_q, w_ret_k, w_ret_v, w_fox_q, w_fox_k, w_fox_v, fox_gates, w_out_ret, w_out_fox
):
    own = lax.all_to_all(jnp.broadcast_to(tokens[None], (4, 32, 2048)), "x", 0, 0, tiled=True)
    other = swapped(own)
    wt = jnp.concatenate([w_out_ret, w_out_fox], axis=0).reshape(3, LANES, 32).transpose(0, 2, 1)
    far = (
        gain.reshape(1, 2048), w_ret_k, w_ret_v, jnp.asarray(ROW_TURN), jnp.asarray(RUN_TURN),
        w_ret_q, w_fox_q, w_fox_k, w_fox_v, fox_gates.reshape(2, LANES),
    )
    m1, states, kvg, qrot, inner = call(
        project_kernel,
        [struct(N, R1, LANES), struct(N, 64, LANES), struct(KG0 + 16, LANES), struct(RUN, RET), struct(RUN, RET, dtype=F32)],
        [pltpu.VMEM((RUN, 2048), BF)] + [pltpu.VMEM(a.shape, a.dtype) for a in far] + [pltpu.SemaphoreType.DMA((len(far),))],
        (own, other, wt), 1_400_000_000, 8_000_000, "project", 60, far,
    )
    m1 = lax.dynamic_update_slice(m1, swapped(states), (0, SB0, 0))
    got1 = exchanged(m1, GROUPS_A)
    (m2,) = call(totals_kernel, [struct(N, R2, LANES)], [], (got1, kvg), 1_000_000, 4_000_000, "totals", 16)
    got2 = exchanged(m2, GROUPS_B)
    (m3,) = call(
        attention_kernel,
        [struct(N, R3, LANES)],
        [pltpu.VMEM((N, RUN, 2 * LANES), BF), pltpu.VMEM((N, RUN, 2 * LANES), BF)],
        (got1, got2), 4_300_000_000, 4_000_000, "attention", 24,
    )
    got3 = exchanged(m3, GROUPS_A)
    sent = swapped(got3[:, CB0 : CB0 + 64, :])
    keep, give = call(
        output_kernel,
        [struct(4, 32, 2048, dtype=F32), struct(4, 32, 2048)],
        [pltpu.VMEM((2048, 384), BF), pltpu.VMEM((RUN, 384), BF), pltpu.VMEM((RET, RET), BF)],
        (got2, got3, sent, qrot, inner), 400_000_000, 4_000_000, "output", 20,
    )
    pair = (keep + swapped(give).astype(F32)).astype(BF)
    return jnp.sum(lax.all_to_all(pair, "x", 0, 0, tiled=True).astype(F32), axis=0).astype(BF)


def solution(mesh):
    split = Mesh(mesh.devices.reshape(N, N, 4, 2), ALL)
    return jax.shard_map(
        per_device,
        mesh=split,
        in_specs=(
            P(ALL, None),
            P(),
            P(None, TP),
            P(None, TP),
            P(None, TP),
            P(None, TP),
            P(None, TP),
            P(None, TP),
            P(SP, TP),
            P(TP, SP),
            P(TP, SP),
        ),
        out_specs=P(ALL, None),
        check_vma=False,
    )
```

```python
import functools
import math

import jax
import jax.numpy as jnp
import numpy as np
from jax import lax
from jax.experimental import pallas as pl
from jax.experimental.pallas import tpu as pltpu
from jax.sharding import Mesh
from jax.sharding import PartitionSpec as P

N = 8
RUN = 256
LANES = 128
RET = 256
FOX = 128
eps = 1e-06
ALL = ("z", "y", "x", "c")
SP = ("z", "y")
TP = ("x", "c")

Q0, QG0, SA0, SB0, W0, R1 = 0, 256, 272, 336, 400, 496
K0, V0, KG0, TA0, TB0, WW0, R2 = 0, 256, 512, 528, 592, 656, 1424
N0, D0, CA0, CB0, R3 = 0, 256, 272, 336, 400

HEADS = np.arange(8, dtype=np.float64)
RATES = np.where(HEADS < 4, 1.0 / (32.0 + 16.0 * HEADS), np.exp2(-(HEADS - 4)) / 16384.0)
PER_RUN = np.exp(-RATES * RUN)
PER_ROW = np.exp(-RATES * RUN * N)
INVERSE = 10000.0 ** (-np.arange(LANES, dtype=np.float64) / LANES)
ROW_ANGLE = np.arange(RUN, dtype=np.float64)[:, None] * INVERSE
RUN_ANGLE = (RUN * np.arange(64, dtype=np.float64))[:, None] * INVERSE
ROW_TURN = np.stack([np.cos(ROW_ANGLE), np.sin(ROW_ANGLE)]).astype(np.float32)
RUN_TURN = np.stack([np.cos(RUN_ANGLE), np.sin(RUN_ANGLE)]).astype(np.float32)

BF = jnp.bfloat16
F32 = jnp.float32


def device_id(z, y, x, c):
    return ((z * N + y) * 4 + x) * 2 + c


Y_GROUPS = [[[device_id(z, y, x, c) for y in range(N)] for z in range(N) for x in range(4)] for c in (0, 1)]
Z_GROUPS = [[[device_id(z, y, x, c) for z in range(N)] for y in range(N) for x in range(4)] for c in (0, 1)]
GROUPS_A = Y_GROUPS[0] + Z_GROUPS[1]
GROUPS_B = Z_GROUPS[0] + Y_GROUPS[1]


def exchanged(message, groups):
    return lax.all_to_all(message, ALL, 0, 0, axis_index_groups=groups, tiled=True)


def swapped(array):
    return lax.ppermute(array, "c", [(0, 1), (1, 0)])


def places():
    z, y, c = lax.axis_index("z"), lax.axis_index("y"), lax.axis_index("c")
    first = c == 0
    return z * N + y, jnp.where(first, y, z), jnp.where(first, z, y), c


def of_head(table, head):
    value = jnp.float32(table[0])
    for h in range(1, 8):
        value = jnp.where(head == h, jnp.float32(table[h]), value)
    return value


def dot_nt(left, right):
    return lax.dot_general(left, right, (((1,), (1,)), ((), ())), preferred_element_type=F32)


def dot_tn(left, right):
    return lax.dot_general(left, right, (((0,), (0,)), ((), ())), preferred_element_type=F32)


def dot(left, right):
    return jnp.dot(left, right, preferred_element_type=F32)


def project_kernel(*refs):
    far, outs = refs[:13], refs[13:18]
    near, made = refs[18:31], refs[31:36]
    xs, in_sems, out_sems = refs[36:]
    copies = [pltpu.make_async_copy(src, dst, in_sems.at[k]) for k, (src, dst) in enumerate(zip(far, near))]
    for copy in copies:
        copy.start()
    own, gain, other, wrk, wrv, row_turn, run_turn, gates, wfq, wt, wrq, wfk, wfv = near
    m1, states, kvg, qrot, inner = made
    stores = [pltpu.make_async_copy(src, dst, out_sems.at[k]) for k, (src, dst) in enumerate(zip(made, outs))]
    place, _, _, c = places()
    rate = of_head(RATES, lax.axis_index("x") * 2 + c)
    copies[0].wait()
    copies[1].wait()
    for part, side in ((own, c), (other, 1 - c)):
        if part is other:
            copies[2].wait()
        for j in range(4):
            x = part[j].astype(F32)
            scaled = x * lax.rsqrt(jnp.mean(x * x, axis=1, keepdims=True) + eps) * gain[...]
            xs[pl.ds(pl.multiple_of(64 * j + 32 * side, 32), 32), :] = scaled.astype(BF)
    x = xs[...]
    for copy in copies[3:7]:
        copy.wait()
    cos_run = run_turn[0, pl.ds(place, 1), :]
    sin_run = run_turn[1, pl.ds(place, 1), :]
    cosine = row_turn[0] * cos_run - row_turn[1] * sin_run
    sine = row_turn[1] * cos_run + row_turn[0] * sin_run

    def turned(values, scale):
        first, second = values[:, :LANES], values[:, LANES:]
        return jnp.concatenate(
            [(first * cosine - second * sine) * scale, (first * sine + second * cosine) * scale], axis=1
        )

    rk = turned(dot(x, wrk[...]).astype(BF).astype(F32), RET**-0.5).astype(BF)
    rv = dot(x, wrv[...]).astype(BF)
    row = lax.broadcasted_iota(jnp.int32, (RUN, RET), 0)
    col = lax.broadcasted_iota(jnp.int32, (RUN, RET), 1)
    kd = (rk.astype(F32) * jnp.exp(-rate * (RUN - 1 - row).astype(F32))).astype(BF)
    state = dot_tn(kd, rv).astype(BF)
    for j in range(N):
        for half in range(2):
            piece = state[32 * j : 32 * j + 32, LANES * half : LANES * half + LANES]
            states[j, 32 * half : 32 * half + 32, :] = piece
            m1[j, SA0 + 32 * half : SA0 + 32 * half + 32, :] = piece
            m1[j, SB0 + 32 * half : SB0 + 32 * half + 32, :] = piece
    stores[1].start()
    for copy in copies[7:10]:
        copy.wait()
    fq = dot(x, wfq[...]).astype(BF)
    line = lax.broadcasted_iota(jnp.int32, (16, LANES), 0)
    gate = jnp.where(line < 8, gates[0:1, :], gates[1:2, :]) * (FOX**0.5)
    high = gate.astype(BF).astype(F32)
    middle = (gate - high).astype(BF).astype(F32)
    low = gate - high - middle
    slot = line & 7
    third = jnp.where(slot == 0, high, jnp.where(slot == 1, middle, low))
    of_query = jnp.where(slot < 3, third, jnp.where(slot < 6, 1.0, 0.0)).astype(BF)
    third = jnp.where(slot == 3, high, jnp.where(slot == 4, middle, low))
    of_key = jnp.where(slot < 3, 1.0, jnp.where(slot < 6, -third, 0.0)).astype(BF)
    for j in range(N):
        m1[j, Q0 : Q0 + RUN, :] = fq
        m1[j, QG0 : QG0 + 16, :] = of_query
        for k in range(3):
            m1[j, W0 + 32 * k : W0 + 32 * k + 32, :] = wt[k]
    stores[0].start()
    for copy in copies[10:]:
        copy.wait()
    kvg[KG0 : KG0 + 16, :] = of_key
    kvg[K0 : K0 + RUN, :] = dot(x, wfk[...]).astype(BF)
    kvg[V0 : V0 + RUN, :] = dot(x, wfv[...]).astype(BF)
    stores[2].start()
    rq = turned(dot(x, wrq[...]).astype(BF).astype(F32), 1.0).astype(BF)
    qrot[...] = rq
    stores[3].start()
    spread = row - col
    within = jnp.where(spread >= 0, jnp.exp(-rate * jnp.maximum(spread, 0).astype(F32)), 0.0)
    inner[...] = dot((dot_nt(rq, rk) * within).astype(BF), rv)
    stores[4].start()
    for store in stores:
        store.wait()


def totals_kernel(got1, kvg, m2):
    head = lax.axis_index("x") * 2 + lax.axis_index("c")
    sums = []
    for start, which in ((SA0, head), (SB0, head ^ 1)):
        decay = of_head(PER_RUN, which)
        total = got1[0, start : start + 64, :].astype(F32)
        for j in range(1, N):
            total = total * decay + got1[j, start : start + 64, :].astype(F32)
        sums.append(total.astype(BF))
    for j in range(N):
        m2[j, 0 : KG0 + 16, :] = kvg[...]
        m2[j, TA0 : TA0 + 64, :] = sums[0]
        m2[j, TB0 : TB0 + 64, :] = sums[1]
        for k in range(N):
            m2[j, WW0 + 96 * k : WW0 + 96 * k + 96, :] = got1[k, W0 : W0 + 96, :]


def as_columns(rows, eye):
    lines = rows.astype(F32)
    wide = jnp.concatenate([lines[0:8], lines[8:16]], axis=1)
    wide = jnp.concatenate([wide, jnp.zeros((LANES - 8, RUN), F32)], axis=0).astype(BF)
    return dot_nt(eye, wide).astype(BF)


def attention_kernel(got1, got2, m3, keys, values):
    _, a, b, c = places()
    head = lax.axis_index("x") * 2 + c
    row = lax.broadcasted_iota(jnp.int32, (RUN, RUN), 0)
    col = lax.broadcasted_iota(jnp.int32, (RUN, RUN), 1)
    eye = jnp.where(row == col, 1.0, 0.0).astype(BF)
    diagonal = (row == col)[:LANES, :LANES]
    ahead = col - row
    for i in range(N):
        keys[i, :, :LANES] = got2[i, K0 : K0 + RUN, :]
        keys[i, :, LANES:] = as_columns(got2[i, KG0 : KG0 + 16, :], eye)
        values[i, :, :LANES] = got2[i, V0 : V0 + RUN, :]
        values[i, :, LANES:] = jnp.ones((RUN, LANES), BF)

    def one_run(j, carry):
        query = jnp.concatenate(
            [got1[j, Q0 : Q0 + RUN, :], as_columns(got1[j, QG0 : QG0 + 16, :], eye)], axis=1
        )
        of_query = jnp.where(c == 0, b * N + j, j * N + b)
        weights = []
        for i in range(N):
            of_key = jnp.where(c == 0, i * N + a, a * N + i)
            score = dot_nt(query, keys[i]) * (FOX**-0.5 * math.log2(math.e))
            score = jnp.where(ahead <= (of_query - of_key) * RUN, score, -jnp.inf)
            weights.append(jnp.exp2(score).astype(BF))
        total = dot(jnp.concatenate(weights, axis=1), values[...].reshape(N * RUN, 2 * LANES))
        m3[j, N0 : N0 + RUN, :] = total[:, :LANES].astype(BF)
        den = [
            jnp.sum(jnp.where(diagonal, total[LANES * h : LANES * h + LANES, LANES:], 0.0), axis=0, keepdims=True)
            for h in range(2)
        ]
        line = lax.broadcasted_iota(jnp.int32, (16, LANES), 0)
        den = jnp.where((line & 1) == 0, den[0], den[1])
        high = den.astype(BF).astype(F32)
        m3[j, D0 : D0 + 16, :] = jnp.where(line < 2, high, jnp.where(line < 4, den - high, 0.0)).astype(BF)
        return carry

    lax.fori_loop(0, N, one_run, 0, unroll=4)
    for own, (sums, slices, carried) in enumerate(((TA0, SA0, CA0), (TB0, SB0, CB0))):
        which = head ^ own
        per_run, per_row = of_head(PER_RUN, which), of_head(PER_ROW, which)
        state = jnp.zeros((64, LANES), F32)
        for k in range(N):
            state = jnp.where(k < b, state * per_row + got2[k, sums : sums + 64, :].astype(F32), state)
        for j in range(N):
            m3[j, carried : carried + 64, :] = state.astype(BF)
            state = state * per_run + got1[j, slices : slices + 64, :].astype(F32)


def output_kernel(got2, got3, sent, qrot, inner, keep, give, weight, mixed, state):
    _, _, _, c = places()
    rate = of_head(RATES, lax.axis_index("x") * 2 + c)
    for i in range(N):
        for k in range(N):
            at = pl.multiple_of(jnp.where(c == 0, i * N + k, k * N + i) * 32, 32)
            for h in range(3):
                start = WW0 + 96 * k + 32 * h
                weight[pl.ds(at, 32), LANES * h : LANES * h + LANES] = got2[i, start : start + 32, :]
    num = got3[0, N0 : N0 + RUN, :].astype(F32)
    den = got3[0, D0 : D0 + 16, :].astype(F32)
    for j in range(1, N):
        num = num + got3[j, N0 : N0 + RUN, :].astype(F32)
        den = den + got3[j, D0 : D0 + 16, :].astype(F32)
    row = lax.broadcasted_iota(jnp.int32, (LANES, LANES), 0)
    col = lax.broadcasted_iota(jnp.int32, (LANES, LANES), 1)
    for h in range(2):
        line = den[h : h + 1, :] + den[h + 2 : h + 3, :]
        column = jnp.sum(jnp.where(row == col, line, 0.0), axis=1, keepdims=True)
        raw = num[LANES * h : LANES * h + LANES] / column
        raw = raw * lax.rsqrt(jnp.mean(raw * raw, axis=1, keepdims=True) + eps)
        mixed[LANES * h : LANES * h + LANES, RET:] = raw.astype(BF)
    for j in range(N):
        for half in range(2):
            start = 32 * half
            piece = jnp.where(
                c == 0, got3[j, CA0 + start : CA0 + start + 32, :].astype(F32), sent[j, start : start + 32, :].astype(F32)
            )
            state[32 * j : 32 * j + 32, LANES * half : LANES * half + LANES] = piece.astype(BF)
    steps = lax.broadcasted_iota(jnp.int32, (RUN, RET), 0)
    raw = inner[...] + dot(qrot[...], state[...]) * jnp.exp(-rate * (steps + 1).astype(F32))
    raw = raw * lax.rsqrt(jnp.mean(raw * raw, axis=1, keepdims=True) + eps)
    mixed[:, :RET] = raw.astype(BF)
    for side, target in ((c, keep), (1 - c, give)):
        rows = jnp.concatenate(
            [mixed[pl.ds(pl.multiple_of(64 * j + 32 * side, 32), 32), :] for j in range(4)], axis=0
        )
        for n in range(4):
            part = dot_nt(rows, weight[512 * n : 512 * n + 512, :])
            for j in range(4):
                target[j, :, 512 * n : 512 * n + 512] = part[32 * j : 32 * j + 32].astype(target.dtype)


def vmem(count):
    return [pl.BlockSpec(memory_space=pltpu.VMEM)] * count


def call(kernel, outs, scratch, args, flops, nbytes, name, limit, far=(), out_space=pltpu.VMEM):
    specs = vmem(len(args)) + [pl.BlockSpec(memory_space=pltpu.HBM)] * len(far)
    return pl.pallas_call(
        kernel,
        out_shape=outs,
        in_specs=specs,
        out_specs=[pl.BlockSpec(memory_space=out_space)] * len(outs),
        scratch_shapes=scratch,
        cost_estimate=pl.CostEstimate(flops=flops, bytes_accessed=nbytes, transcendentals=0),
        compiler_params=pltpu.CompilerParams(vmem_limit_bytes=limit << 20),
        name=name,
    )(*args, *far)


def struct(*shape, dtype=BF):
    return jax.ShapeDtypeStruct(shape, dtype)


def per_device(
    tokens, gain, w_ret_q, w_ret_k, w_ret_v, w_fox_q, w_fox_k, w_fox_v, fox_gates, w_out_ret, w_out_fox
):
    own = lax.all_to_all(jnp.broadcast_to(tokens[None], (4, 32, 2048)), "x", 0, 0, tiled=True)
    other = swapped(own)
    wt = jnp.concatenate([w_out_ret, w_out_fox], axis=0).reshape(3, LANES, 32).transpose(0, 2, 1)
    far = (
        own, gain.reshape(1, 2048), other, w_ret_k, w_ret_v, jnp.asarray(ROW_TURN), jnp.asarray(RUN_TURN),
        fox_gates.reshape(2, LANES), w_fox_q, wt, w_ret_q, w_fox_k, w_fox_v,
    )
    made = [struct(N, R1, LANES), struct(N, 64, LANES), struct(KG0 + 16, LANES), struct(RUN, RET), struct(RUN, RET, dtype=F32)]
    m1, states, kvg, qrot, inner = call(
        project_kernel,
        made,
        [pltpu.VMEM(a.shape, a.dtype) for a in (*far, *made)]
        + [pltpu.VMEM((RUN, 2048), BF), pltpu.SemaphoreType.DMA((len(far),)), pltpu.SemaphoreType.DMA((len(made),))],
        (), 1_400_000_000, 8_000_000, "project", 60, far, pltpu.HBM,
    )
    m1 = lax.dynamic_update_slice(m1, swapped(states), (0, SB0, 0))
    got1 = exchanged(m1, GROUPS_A)
    (m2,) = call(totals_kernel, [struct(N, R2, LANES)], [], (got1, kvg), 1_000_000, 4_000_000, "totals", 16)
    got2 = exchanged(m2, GROUPS_B)
    (m3,) = call(
        attention_kernel,
        [struct(N, R3, LANES)],
        [pltpu.VMEM((N, RUN, 2 * LANES), BF), pltpu.VMEM((N, RUN, 2 * LANES), BF)],
        (got1, got2), 4_300_000_000, 4_000_000, "attention", 24,
    )
    got3 = exchanged(m3, GROUPS_A)
    sent = swapped(got3[:, CB0 : CB0 + 64, :])
    keep, give = call(
        output_kernel,
        [struct(4, 32, 2048, dtype=F32), struct(4, 32, 2048)],
        [pltpu.VMEM((2048, 384), BF), pltpu.VMEM((RUN, 384), BF), pltpu.VMEM((RET, RET), BF)],
        (got2, got3, sent, qrot, inner), 400_000_000, 4_000_000, "output", 20,
    )
    pair = (keep + swapped(give).astype(F32)).astype(BF)
    return jnp.sum(lax.all_to_all(pair, "x", 0, 0, tiled=True).astype(F32), axis=0).astype(BF)


def solution(mesh):
    split = Mesh(mesh.devices.reshape(N, N, 4, 2), ALL)
    return jax.shard_map(
        per_device,
        mesh=split,
        in_specs=(
            P(ALL, None),
            P(),
            P(None, TP),
            P(None, TP),
            P(None, TP),
            P(None, TP),
            P(None, TP),
            P(None, TP),
            P(SP, TP),
            P(TP, SP),
            P(TP, SP),
        ),
        out_specs=P(ALL, None),
        check_vma=False,
    )
```

```python
import functools
import math

import jax
import jax.numpy as jnp
import numpy as np
from jax import lax
from jax.experimental import pallas as pl
from jax.experimental.pallas import tpu as pltpu
from jax.sharding import Mesh
from jax.sharding import PartitionSpec as P

N = 8
RUN = 256
LANES = 128
RET = 256
FOX = 128
eps = 1e-06
ALL = ("z", "y", "x", "c")
SP = ("z", "y")
TP = ("x", "c")

Q0, QG0, SA0, SB0, W0, R1 = 0, 256, 272, 336, 400, 480
K0, V0, KG0, TA0, TB0, WW0, R2 = 0, 256, 512, 528, 592, 656, 1312
N0, D0, CA0, CB0, R3 = 0, 256, 272, 336, 400
SPARE = 1296

HEADS = np.arange(8, dtype=np.float64)
RATES = np.where(HEADS < 4, 1.0 / (32.0 + 16.0 * HEADS), np.exp2(-(HEADS - 4)) / 16384.0)
PER_RUN = np.exp(-RATES * RUN)
PER_ROW = np.exp(-RATES * RUN * N)
INVERSE = 10000.0 ** (-np.arange(LANES, dtype=np.float64) / LANES)
ROW_ANGLE = np.arange(RUN, dtype=np.float64)[:, None] * INVERSE
RUN_ANGLE = (RUN * np.arange(64, dtype=np.float64))[:, None] * INVERSE
ROW_TURN = np.stack([np.cos(ROW_ANGLE), np.sin(ROW_ANGLE)]).astype(np.float32)
RUN_TURN = np.stack([np.cos(RUN_ANGLE), np.sin(RUN_ANGLE)]).astype(np.float32)

BF = jnp.bfloat16
F32 = jnp.float32


def device_id(z, y, x, c):
    return ((z * N + y) * 4 + x) * 2 + c


Y_GROUPS = [[[device_id(z, y, x, c) for y in range(N)] for z in range(N) for x in range(4)] for c in (0, 1)]
Z_GROUPS = [[[device_id(z, y, x, c) for z in range(N)] for y in range(N) for x in range(4)] for c in (0, 1)]
GROUPS_A = Y_GROUPS[0] + Z_GROUPS[1]
GROUPS_B = Z_GROUPS[0] + Y_GROUPS[1]


def exchanged(message, groups):
    return lax.all_to_all(message, ALL, 0, 0, axis_index_groups=groups, tiled=True)


def swapped(array):
    return lax.ppermute(array, "c", [(0, 1), (1, 0)])


def places():
    z, y, c = lax.axis_index("z"), lax.axis_index("y"), lax.axis_index("c")
    first = c == 0
    return z * N + y, jnp.where(first, y, z), jnp.where(first, z, y), c


def of_head(table, head):
    value = jnp.float32(table[0])
    for h in range(1, 8):
        value = jnp.where(head == h, jnp.float32(table[h]), value)
    return value


def dot_nt(left, right):
    return lax.dot_general(left, right, (((1,), (1,)), ((), ())), preferred_element_type=F32)


def dot_tn(left, right):
    return lax.dot_general(left, right, (((0,), (0,)), ((), ())), preferred_element_type=F32)


def dot(left, right):
    return jnp.dot(left, right, preferred_element_type=F32)


def project_kernel(*refs):
    far, outs = refs[:13], refs[13:18]
    near, made = refs[18:31], refs[31:36]
    xs, in_sems, out_sems = refs[36:]
    copies = [pltpu.make_async_copy(src, dst, in_sems.at[k]) for k, (src, dst) in enumerate(zip(far, near))]
    for copy in copies:
        copy.start()
    own, gain, other, wrk, wrv, row_turn, run_turn, gates, wfq, wt, wrq, wfk, wfv = near
    m1, states, kvg, qrot, inner = made
    stores = [pltpu.make_async_copy(src, dst, out_sems.at[k]) for k, (src, dst) in enumerate(zip(made, outs))]
    place, _, _, c = places()
    rate = of_head(RATES, lax.axis_index("x") * 2 + c)
    copies[0].wait()
    copies[1].wait()
    for part, side in ((own, c), (other, 1 - c)):
        if part is other:
            copies[2].wait()
        for j in range(4):
            x = part[j].astype(F32)
            scaled = x * lax.rsqrt(jnp.mean(x * x, axis=1, keepdims=True) + eps) * gain[...]
            xs[pl.ds(pl.multiple_of(64 * j + 32 * side, 32), 32), :] = scaled.astype(BF)
    x = xs[...]
    for copy in copies[3:7]:
        copy.wait()
    cos_run = run_turn[0, pl.ds(place, 1), :]
    sin_run = run_turn[1, pl.ds(place, 1), :]
    cosine = row_turn[0] * cos_run - row_turn[1] * sin_run
    sine = row_turn[1] * cos_run + row_turn[0] * sin_run

    def turned(values, scale):
        first, second = values[:, :LANES], values[:, LANES:]
        return jnp.concatenate(
            [(first * cosine - second * sine) * scale, (first * sine + second * cosine) * scale], axis=1
        )

    rk = turned(dot(x, wrk[...]).astype(BF).astype(F32), RET**-0.5).astype(BF)
    rv = dot(x, wrv[...]).astype(BF)
    row = lax.broadcasted_iota(jnp.int32, (RUN, RET), 0)
    col = lax.broadcasted_iota(jnp.int32, (RUN, RET), 1)
    kd = (rk.astype(F32) * jnp.exp(-rate * (RUN - 1 - row).astype(F32))).astype(BF)
    state = dot_tn(kd, rv).astype(BF)
    for j in range(N):
        for half in range(2):
            piece = state[32 * j : 32 * j + 32, LANES * half : LANES * half + LANES]
            states[j, 32 * half : 32 * half + 32, :] = piece
    for copy in copies[7:10]:
        copy.wait()

    @pl.when(c == 0)
    def _():
        for j in range(N):
            m1[j, SA0 : SA0 + 64, :] = states[j]
            m1[j, W0 : W0 + 32, :] = wt[0]
            m1[j, W0 + 32 : W0 + 64, :] = wt[1]
            m1[j, W0 + 64 : W0 + 80, :] = wt[2, 0:16, :]
        states[0, 0:16, :] = wt[2, 16:32, :]

    @pl.when(c == 1)
    def _():
        for j in range(N):
            m1[j, SA0 : SA0 + 32, :] = wt[0]
            m1[j, SA0 + 32 : SA0 + 64, :] = wt[1]
            m1[j, W0 : W0 + 32, :] = wt[2]
            m1[j, W0 + 32 : W0 + 80, :] = jnp.zeros((48, LANES), BF)

    stores[1].start()
    fq = dot(x, wfq[...]).astype(BF)
    line = lax.broadcasted_iota(jnp.int32, (16, LANES), 0)
    gate = jnp.where(line < 8, gates[0:1, :], gates[1:2, :]) * (FOX**0.5)
    high = gate.astype(BF).astype(F32)
    middle = (gate - high).astype(BF).astype(F32)
    low = gate - high - middle
    slot = line & 7
    third = jnp.where(slot == 0, high, jnp.where(slot == 1, middle, low))
    of_query = jnp.where(slot < 3, third, jnp.where(slot < 6, 1.0, 0.0)).astype(BF)
    third = jnp.where(slot == 3, high, jnp.where(slot == 4, middle, low))
    of_key = jnp.where(slot < 3, 1.0, jnp.where(slot < 6, -third, 0.0)).astype(BF)
    for j in range(N):
        m1[j, Q0 : Q0 + RUN, :] = fq
        m1[j, QG0 : QG0 + 16, :] = of_query
        m1[j, SB0 : SB0 + 64, :] = jnp.zeros((64, LANES), BF)
    stores[0].start()
    for copy in copies[10:]:
        copy.wait()
    kvg[KG0 : KG0 + 16, :] = of_key
    kvg[K0 : K0 + RUN, :] = dot(x, wfk[...]).astype(BF)
    kvg[V0 : V0 + RUN, :] = dot(x, wfv[...]).astype(BF)
    stores[2].start()
    rq = turned(dot(x, wrq[...]).astype(BF).astype(F32), 1.0).astype(BF)
    qrot[...] = rq
    stores[3].start()
    spread = row - col
    within = jnp.where(spread >= 0, jnp.exp(-rate * jnp.maximum(spread, 0).astype(F32)), 0.0)
    inner[...] = dot((dot_nt(rq, rk) * within).astype(BF), rv)
    stores[4].start()
    for store in stores:
        store.wait()


def totals_kernel(got1, kvg, spare, m2):
    c = lax.axis_index("c")
    head = lax.axis_index("x") * 2 + c
    for j in range(N):
        m2[j, 0 : KG0 + 16, :] = kvg[...]

    @pl.when(c == 0)
    def _():
        sums = []
        for start, which in ((SA0, head), (SB0, head ^ 1)):
            decay = of_head(PER_RUN, which)
            total = got1[0, start : start + 64, :].astype(F32)
            for j in range(1, N):
                total = total * decay + got1[j, start : start + 64, :].astype(F32)
            sums.append(total.astype(BF))
        for j in range(N):
            m2[j, TA0 : TA0 + 64, :] = sums[0]
            m2[j, TB0 : TB0 + 64, :] = sums[1]
            for k in range(N):
                m2[j, WW0 + 80 * k : WW0 + 80 * k + 80, :] = got1[k, W0 : W0 + 80, :]
            m2[j, SPARE : SPARE + 16, :] = jnp.zeros((16, LANES), BF)

    @pl.when(c == 1)
    def _():
        for j in range(N):
            for k in range(N):
                m2[j, TA0 + 96 * k : TA0 + 96 * k + 64, :] = got1[k, SA0 : SA0 + 64, :]
                m2[j, TA0 + 96 * k + 64 : TA0 + 96 * k + 96, :] = got1[k, W0 : W0 + 32, :]
            m2[j, SPARE : SPARE + 16, :] = spare[0, 0:16, :]


def as_columns(rows, eye):
    lines = rows.astype(F32)
    wide = jnp.concatenate([lines[0:8], lines[8:16]], axis=1)
    wide = jnp.concatenate([wide, jnp.zeros((LANES - 8, RUN), F32)], axis=0).astype(BF)
    return dot_nt(eye, wide).astype(BF)


def attention_kernel(got1, got2, m3, keys, values):
    _, a, b, c = places()
    head = lax.axis_index("x") * 2 + c
    row = lax.broadcasted_iota(jnp.int32, (RUN, RUN), 0)
    col = lax.broadcasted_iota(jnp.int32, (RUN, RUN), 1)
    eye = jnp.where(row == col, 1.0, 0.0).astype(BF)
    diagonal = (row == col)[:LANES, :LANES]
    ahead = col - row
    for i in range(N):
        keys[i, :, :LANES] = got2[i, K0 : K0 + RUN, :]
        keys[i, :, LANES:] = as_columns(got2[i, KG0 : KG0 + 16, :], eye)
        values[i, :, :LANES] = got2[i, V0 : V0 + RUN, :]
        values[i, :, LANES:] = jnp.ones((RUN, LANES), BF)

    def one_run(j, carry):
        query = jnp.concatenate(
            [got1[j, Q0 : Q0 + RUN, :], as_columns(got1[j, QG0 : QG0 + 16, :], eye)], axis=1
        )
        of_query = jnp.where(c == 0, b * N + j, j * N + b)
        weights = []
        for i in range(N):
            of_key = jnp.where(c == 0, i * N + a, a * N + i)
            score = dot_nt(query, keys[i]) * (FOX**-0.5 * math.log2(math.e))
            score = jnp.where(ahead <= (of_query - of_key) * RUN, score, -jnp.inf)
            weights.append(jnp.exp2(score).astype(BF))
        total = dot(jnp.concatenate(weights, axis=1), values[...].reshape(N * RUN, 2 * LANES))
        m3[j, N0 : N0 + RUN, :] = total[:, :LANES].astype(BF)
        den = [
            jnp.sum(jnp.where(diagonal, total[LANES * h : LANES * h + LANES, LANES:], 0.0), axis=0, keepdims=True)
            for h in range(2)
        ]
        line = lax.broadcasted_iota(jnp.int32, (16, LANES), 0)
        den = jnp.where((line & 1) == 0, den[0], den[1])
        high = den.astype(BF).astype(F32)
        m3[j, D0 : D0 + 16, :] = jnp.where(line < 2, high, jnp.where(line < 4, den - high, 0.0)).astype(BF)
        return carry

    lax.fori_loop(0, N, one_run, 0, unroll=4)
    @pl.when(c == 0)
    def _():
        for own, (sums, slices, carried) in enumerate(((TA0, SA0, CA0), (TB0, SB0, CB0))):
            which = head ^ own
            per_run, per_row = of_head(PER_RUN, which), of_head(PER_ROW, which)
            state = jnp.zeros((64, LANES), F32)
            for k in range(N):
                state = jnp.where(k < b, state * per_row + got2[k, sums : sums + 64, :].astype(F32), state)
            for j in range(N):
                m3[j, carried : carried + 64, :] = state.astype(BF)
                state = state * per_run + got1[j, slices : slices + 64, :].astype(F32)

    @pl.when(c == 1)
    def _():
        for j in range(N):
            for i in range(N):
                m3[j, CA0 + 16 * i : CA0 + 16 * i + 16, :] = got2[i, SPARE : SPARE + 16, :]


def output_kernel(got2, got3, sent, qrot, inner, keep, give, weight, mixed, state):
    _, _, _, c = places()
    rate = of_head(RATES, lax.axis_index("x") * 2 + c)
    @pl.when(c == 0)
    def _():
        for i in range(N):
            for k in range(N):
                at, start = (i * N + k) * 32, WW0 + 80 * k
                weight[at : at + 32, :LANES] = got2[i, start : start + 32, :]
                weight[at : at + 32, LANES : 2 * LANES] = got2[i, start + 32 : start + 64, :]
                weight[at : at + 16, 2 * LANES :] = got2[i, start + 64 : start + 80, :]
                at = (k * N + i) * 32
                weight[at + 16 : at + 32, 2 * LANES :] = sent[k, 16 * i : 16 * i + 16, :]
        for j in range(N):
            for half in range(2):
                piece = got3[j, CA0 + 32 * half : CA0 + 32 * half + 32, :]
                state[32 * j : 32 * j + 32, LANES * half : LANES * half + LANES] = piece

    @pl.when(c == 1)
    def _():
        for i in range(N):
            for k in range(N):
                at, start = (k * N + i) * 32, TA0 + 96 * k
                for h in range(3):
                    weight[at : at + 32, LANES * h : LANES * h + LANES] = got2[i, start + 32 * h : start + 32 * h + 32, :]
        for j in range(N):
            for half in range(2):
                piece = sent[j, 64 + 32 * half : 64 + 32 * half + 32, :]
                state[32 * j : 32 * j + 32, LANES * half : LANES * half + LANES] = piece

    num = got3[0, N0 : N0 + RUN, :].astype(F32)
    den = got3[0, D0 : D0 + 16, :].astype(F32)
    for j in range(1, N):
        num = num + got3[j, N0 : N0 + RUN, :].astype(F32)
        den = den + got3[j, D0 : D0 + 16, :].astype(F32)
    row = lax.broadcasted_iota(jnp.int32, (LANES, LANES), 0)
    col = lax.broadcasted_iota(jnp.int32, (LANES, LANES), 1)
    for h in range(2):
        line = den[h : h + 1, :] + den[h + 2 : h + 3, :]
        column = jnp.sum(jnp.where(row == col, line, 0.0), axis=1, keepdims=True)
        raw = num[LANES * h : LANES * h + LANES] / column
        raw = raw * lax.rsqrt(jnp.mean(raw * raw, axis=1, keepdims=True) + eps)
        mixed[LANES * h : LANES * h + LANES, RET:] = raw.astype(BF)
    steps = lax.broadcasted_iota(jnp.int32, (RUN, RET), 0)
    raw = inner[...] + dot(qrot[...], state[...]) * jnp.exp(-rate * (steps + 1).astype(F32))
    raw = raw * lax.rsqrt(jnp.mean(raw * raw, axis=1, keepdims=True) + eps)
    mixed[:, :RET] = raw.astype(BF)
    for side, target in ((c, keep), (1 - c, give)):
        rows = jnp.concatenate(
            [mixed[pl.ds(pl.multiple_of(64 * j + 32 * side, 32), 32), :] for j in range(4)], axis=0
        )
        for n in range(4):
            part = dot_nt(rows, weight[512 * n : 512 * n + 512, :])
            for j in range(4):
                target[j, :, 512 * n : 512 * n + 512] = part[32 * j : 32 * j + 32].astype(target.dtype)


def vmem(count):
    return [pl.BlockSpec(memory_space=pltpu.VMEM)] * count


def call(kernel, outs, scratch, args, flops, nbytes, name, limit, far=(), out_space=pltpu.VMEM):
    specs = vmem(len(args)) + [pl.BlockSpec(memory_space=pltpu.HBM)] * len(far)
    return pl.pallas_call(
        kernel,
        out_shape=outs,
        in_specs=specs,
        out_specs=[pl.BlockSpec(memory_space=out_space)] * len(outs),
        scratch_shapes=scratch,
        cost_estimate=pl.CostEstimate(flops=flops, bytes_accessed=nbytes, transcendentals=0),
        compiler_params=pltpu.CompilerParams(vmem_limit_bytes=limit << 20),
        name=name,
    )(*args, *far)


def struct(*shape, dtype=BF):
    return jax.ShapeDtypeStruct(shape, dtype)


def per_device(
    tokens, gain, w_ret_q, w_ret_k, w_ret_v, w_fox_q, w_fox_k, w_fox_v, fox_gates, w_out_ret, w_out_fox
):
    own = lax.all_to_all(jnp.broadcast_to(tokens[None], (4, 32, 2048)), "x", 0, 0, tiled=True)
    other = swapped(own)
    wt = jnp.concatenate([w_out_ret, w_out_fox], axis=0).reshape(3, LANES, 32).transpose(0, 2, 1)
    far = (
        own, gain.reshape(1, 2048), other, w_ret_k, w_ret_v, jnp.asarray(ROW_TURN), jnp.asarray(RUN_TURN),
        fox_gates.reshape(2, LANES), w_fox_q, wt, w_ret_q, w_fox_k, w_fox_v,
    )
    made = [struct(N, R1, LANES), struct(N, 64, LANES), struct(KG0 + 16, LANES), struct(RUN, RET), struct(RUN, RET, dtype=F32)]
    m1, states, kvg, qrot, inner = call(
        project_kernel,
        made,
        [pltpu.VMEM(a.shape, a.dtype) for a in (*far, *made)]
        + [pltpu.VMEM((RUN, 2048), BF), pltpu.SemaphoreType.DMA((len(far),)), pltpu.SemaphoreType.DMA((len(made),))],
        (), 1_400_000_000, 8_000_000, "project", 60, far, pltpu.HBM,
    )
    spare = swapped(states)
    m1 = lax.dynamic_update_slice(m1, spare, (0, SB0, 0))
    got1 = exchanged(m1, GROUPS_A)
    (m2,) = call(totals_kernel, [struct(N, R2, LANES)], [], (got1, kvg, spare), 1_000_000, 4_000_000, "totals", 16)
    got2 = exchanged(m2, GROUPS_B)
    (m3,) = call(
        attention_kernel,
        [struct(N, R3, LANES)],
        [pltpu.VMEM((N, RUN, 2 * LANES), BF), pltpu.VMEM((N, RUN, 2 * LANES), BF)],
        (got1, got2), 4_300_000_000, 4_000_000, "attention", 24,
    )
    got3 = exchanged(m3, GROUPS_A)
    sent = swapped(got3[:, CA0 : CA0 + 128, :])
    keep, give = call(
        output_kernel,
        [struct(4, 32, 2048, dtype=F32), struct(4, 32, 2048)],
        [pltpu.VMEM((2048, 384), BF), pltpu.VMEM((RUN, 384), BF), pltpu.VMEM((RET, RET), BF)],
        (got2, got3, sent, qrot, inner), 400_000_000, 4_000_000, "output", 20,
    )
    pair = (keep + swapped(give).astype(F32)).astype(BF)
    return jnp.sum(lax.all_to_all(pair, "x", 0, 0, tiled=True).astype(F32), axis=0).astype(BF)


def solution(mesh):
    split = Mesh(mesh.devices.reshape(N, N, 4, 2), ALL)
    return jax.shard_map(
        per_device,
        mesh=split,
        in_specs=(
            P(ALL, None),
            P(),
            P(None, TP),
            P(None, TP),
            P(None, TP),
            P(None, TP),
            P(None, TP),
            P(None, TP),
            P(SP, TP),
            P(TP, SP),
            P(TP, SP),
        ),
        out_specs=P(ALL, None),
        check_vma=False,
    )
```

```python
import functools
import math

import jax
import jax.numpy as jnp
import numpy as np
from jax import lax
from jax.experimental import pallas as pl
from jax.experimental.pallas import tpu as pltpu
from jax.sharding import Mesh
from jax.sharding import PartitionSpec as P

N = 8
RUN = 256
LANES = 128
RET = 256
FOX = 128
eps = 1e-06
ALL = ("z", "y", "x", "c")
SP = ("z", "y")
TP = ("x", "c")

Q0, QG0, SA0, SB0, W0, R1 = 0, 256, 272, 336, 400, 480
K0, V0, KG0, TA0, TB0, WW0, R2 = 0, 256, 512, 528, 592, 656, 1312
N0, D0, CA0, CB0, R3 = 0, 256, 272, 336, 400
SPARE = 1296

HEADS = np.arange(8, dtype=np.float64)
RATES = np.where(HEADS < 4, 1.0 / (32.0 + 16.0 * HEADS), np.exp2(-(HEADS - 4)) / 16384.0)
PER_RUN = np.exp(-RATES * RUN)
PER_ROW = np.exp(-RATES * RUN * N)
INVERSE = 10000.0 ** (-np.arange(LANES, dtype=np.float64) / LANES)
ROW_ANGLE = np.arange(RUN, dtype=np.float64)[:, None] * INVERSE
RUN_ANGLE = (RUN * np.arange(64, dtype=np.float64))[:, None] * INVERSE
ROW_TURN = np.stack([np.cos(ROW_ANGLE), np.sin(ROW_ANGLE)]).astype(np.float32)
RUN_TURN = np.stack([np.cos(RUN_ANGLE), np.sin(RUN_ANGLE)]).astype(np.float32)

BF = jnp.bfloat16
F32 = jnp.float32


def device_id(z, y, x, c):
    return ((z * N + y) * 4 + x) * 2 + c


Y_GROUPS = [[[device_id(z, y, x, c) for y in range(N)] for z in range(N) for x in range(4)] for c in (0, 1)]
Z_GROUPS = [[[device_id(z, y, x, c) for z in range(N)] for y in range(N) for x in range(4)] for c in (0, 1)]
GROUPS_A = Y_GROUPS[0] + Z_GROUPS[1]
GROUPS_B = Z_GROUPS[0] + Y_GROUPS[1]


def exchanged(message, groups):
    return lax.all_to_all(message, ALL, 0, 0, axis_index_groups=groups, tiled=True)


def swapped(array):
    return lax.ppermute(array, "c", [(0, 1), (1, 0)])


def places():
    z, y, c = lax.axis_index("z"), lax.axis_index("y"), lax.axis_index("c")
    first = c == 0
    return z * N + y, jnp.where(first, y, z), jnp.where(first, z, y), c


def of_head(table, head):
    value = jnp.float32(table[0])
    for h in range(1, 8):
        value = jnp.where(head == h, jnp.float32(table[h]), value)
    return value


def dot_nt(left, right):
    return lax.dot_general(left, right, (((1,), (1,)), ((), ())), preferred_element_type=F32)


def dot_tn(left, right):
    return lax.dot_general(left, right, (((0,), (0,)), ((), ())), preferred_element_type=F32)


def dot(left, right):
    return jnp.dot(left, right, preferred_element_type=F32)


def turned(values, cosine, sine, scale):
    first, second = values[:, :LANES], values[:, LANES:]
    return jnp.concatenate(
        [(first * cosine - second * sine) * scale, (first * sine + second * cosine) * scale], axis=1
    )


def project_kernel(*refs):
    far, outs = refs[:10], refs[10:17]
    near, made = refs[17:27], refs[27:34]
    in_sems, out_sems = refs[34:]
    copies = [pltpu.make_async_copy(src, dst, in_sems.at[k]) for k, (src, dst) in enumerate(zip(far, near))]
    for copy in copies:
        copy.start()
    own, gain, other, wrk, wrv, row_turn, run_turn, gates, wfq, wt = near
    m1, states, xs, turn, rkeys, rvalues, kgates = made
    stores = [pltpu.make_async_copy(src, dst, out_sems.at[k]) for k, (src, dst) in enumerate(zip(made, outs))]
    place, _, _, c = places()
    rate = of_head(RATES, lax.axis_index("x") * 2 + c)
    copies[0].wait()
    copies[1].wait()
    for part, side in ((own, c), (other, 1 - c)):
        if part is other:
            copies[2].wait()
        for j in range(4):
            x = part[j].astype(F32)
            scaled = x * lax.rsqrt(jnp.mean(x * x, axis=1, keepdims=True) + eps) * gain[...]
            xs[pl.ds(pl.multiple_of(64 * j + 32 * side, 32), 32), :] = scaled.astype(BF)
    stores[2].start()
    x = xs[...]
    for copy in copies[3:7]:
        copy.wait()
    cos_run = run_turn[0, pl.ds(place, 1), :]
    sin_run = run_turn[1, pl.ds(place, 1), :]
    cosine = row_turn[0] * cos_run - row_turn[1] * sin_run
    sine = row_turn[1] * cos_run + row_turn[0] * sin_run
    turn[0] = cosine
    turn[1] = sine
    stores[3].start()
    rk = turned(dot(x, wrk[...]).astype(BF).astype(F32), cosine, sine, RET**-0.5).astype(BF)
    rv = dot(x, wrv[...]).astype(BF)
    rkeys[...] = rk
    rvalues[...] = rv
    stores[4].start()
    stores[5].start()
    row = lax.broadcasted_iota(jnp.int32, (RUN, RET), 0)
    col = lax.broadcasted_iota(jnp.int32, (RUN, RET), 1)
    kd = (rk.astype(F32) * jnp.exp(-rate * (RUN - 1 - row).astype(F32))).astype(BF)
    state = dot_tn(kd, rv).astype(BF)
    for j in range(N):
        for half in range(2):
            piece = state[32 * j : 32 * j + 32, LANES * half : LANES * half + LANES]
            states[j, 32 * half : 32 * half + 32, :] = piece
    for copy in copies[7:10]:
        copy.wait()

    @pl.when(c == 0)
    def _():
        for j in range(N):
            m1[j, SA0 : SA0 + 64, :] = states[j]
            m1[j, W0 : W0 + 32, :] = wt[0]
            m1[j, W0 + 32 : W0 + 64, :] = wt[1]
            m1[j, W0 + 64 : W0 + 80, :] = wt[2, 0:16, :]
        states[0, 0:16, :] = wt[2, 16:32, :]

    @pl.when(c == 1)
    def _():
        for j in range(N):
            m1[j, SA0 : SA0 + 32, :] = wt[0]
            m1[j, SA0 + 32 : SA0 + 64, :] = wt[1]
            m1[j, W0 : W0 + 32, :] = wt[2]
            m1[j, W0 + 32 : W0 + 80, :] = jnp.zeros((48, LANES), BF)

    stores[1].start()
    fq = dot(x, wfq[...]).astype(BF)
    line = lax.broadcasted_iota(jnp.int32, (16, LANES), 0)
    gate = jnp.where(line < 8, gates[0:1, :], gates[1:2, :]) * (FOX**0.5)
    high = gate.astype(BF).astype(F32)
    middle = (gate - high).astype(BF).astype(F32)
    low = gate - high - middle
    slot = line & 7
    third = jnp.where(slot == 0, high, jnp.where(slot == 1, middle, low))
    of_query = jnp.where(slot < 3, third, jnp.where(slot < 6, 1.0, 0.0)).astype(BF)
    third = jnp.where(slot == 3, high, jnp.where(slot == 4, middle, low))
    of_key = jnp.where(slot < 3, 1.0, jnp.where(slot < 6, -third, 0.0)).astype(BF)
    for j in range(N):
        m1[j, Q0 : Q0 + RUN, :] = fq
        m1[j, QG0 : QG0 + 16, :] = of_query
        m1[j, SB0 : SB0 + 64, :] = jnp.zeros((64, LANES), BF)
    stores[0].start()
    kgates[...] = of_key
    stores[6].start()
    for store in stores:
        store.wait()


def rest_kernel(xs, turn, rkeys, rvalues, kgates, wrq, wfk, wfv, kvg, qrot, inner):
    rate = of_head(RATES, lax.axis_index("x") * 2 + lax.axis_index("c"))
    x = xs[...]
    kvg[KG0 : KG0 + 16, :] = kgates[...]
    kvg[K0 : K0 + RUN, :] = dot(x, wfk[...]).astype(BF)
    kvg[V0 : V0 + RUN, :] = dot(x, wfv[...]).astype(BF)
    rq = turned(dot(x, wrq[...]).astype(BF).astype(F32), turn[0], turn[1], 1.0).astype(BF)
    qrot[...] = rq
    row = lax.broadcasted_iota(jnp.int32, (RUN, RET), 0)
    spread = row - lax.broadcasted_iota(jnp.int32, (RUN, RET), 1)
    within = jnp.where(spread >= 0, jnp.exp(-rate * jnp.maximum(spread, 0).astype(F32)), 0.0)
    inner[...] = dot((dot_nt(rq, rkeys[...]) * within).astype(BF), rvalues[...])


def totals_kernel(got1, kvg, spare, m2):
    c = lax.axis_index("c")
    head = lax.axis_index("x") * 2 + c
    for j in range(N):
        m2[j, 0 : KG0 + 16, :] = kvg[...]

    @pl.when(c == 0)
    def _():
        sums = []
        for start, which in ((SA0, head), (SB0, head ^ 1)):
            decay = of_head(PER_RUN, which)
            total = got1[0, start : start + 64, :].astype(F32)
            for j in range(1, N):
                total = total * decay + got1[j, start : start + 64, :].astype(F32)
            sums.append(total.astype(BF))
        for j in range(N):
            m2[j, TA0 : TA0 + 64, :] = sums[0]
            m2[j, TB0 : TB0 + 64, :] = sums[1]
            for k in range(N):
                m2[j, WW0 + 80 * k : WW0 + 80 * k + 80, :] = got1[k, W0 : W0 + 80, :]
            m2[j, SPARE : SPARE + 16, :] = jnp.zeros((16, LANES), BF)

    @pl.when(c == 1)
    def _():
        for j in range(N):
            for k in range(N):
                m2[j, TA0 + 96 * k : TA0 + 96 * k + 64, :] = got1[k, SA0 : SA0 + 64, :]
                m2[j, TA0 + 96 * k + 64 : TA0 + 96 * k + 96, :] = got1[k, W0 : W0 + 32, :]
            m2[j, SPARE : SPARE + 16, :] = spare[0, 0:16, :]


def as_columns(rows, eye):
    lines = rows.astype(F32)
    wide = jnp.concatenate([lines[0:8], lines[8:16]], axis=1)
    wide = jnp.concatenate([wide, jnp.zeros((LANES - 8, RUN), F32)], axis=0).astype(BF)
    return dot_nt(eye, wide).astype(BF)


def attention_kernel(got1, got2, m3, keys, values):
    _, a, b, c = places()
    head = lax.axis_index("x") * 2 + c
    row = lax.broadcasted_iota(jnp.int32, (RUN, RUN), 0)
    col = lax.broadcasted_iota(jnp.int32, (RUN, RUN), 1)
    eye = jnp.where(row == col, 1.0, 0.0).astype(BF)
    diagonal = (row == col)[:LANES, :LANES]
    ahead = col - row
    for i in range(N):
        keys[i, :, :LANES] = got2[i, K0 : K0 + RUN, :]
        keys[i, :, LANES:] = as_columns(got2[i, KG0 : KG0 + 16, :], eye)
        values[i, :, :LANES] = got2[i, V0 : V0 + RUN, :]
        values[i, :, LANES:] = jnp.ones((RUN, LANES), BF)

    def one_run(j, carry):
        query = jnp.concatenate(
            [got1[j, Q0 : Q0 + RUN, :], as_columns(got1[j, QG0 : QG0 + 16, :], eye)], axis=1
        )
        of_query = jnp.where(c == 0, b * N + j, j * N + b)
        weights = []
        for i in range(N):
            of_key = jnp.where(c == 0, i * N + a, a * N + i)
            score = dot_nt(query, keys[i]) * (FOX**-0.5 * math.log2(math.e))
            score = jnp.where(ahead <= (of_query - of_key) * RUN, score, -jnp.inf)
            weights.append(jnp.exp2(score).astype(BF))
        total = dot(jnp.concatenate(weights, axis=1), values[...].reshape(N * RUN, 2 * LANES))
        m3[j, N0 : N0 + RUN, :] = total[:, :LANES].astype(BF)
        den = [
            jnp.sum(jnp.where(diagonal, total[LANES * h : LANES * h + LANES, LANES:], 0.0), axis=0, keepdims=True)
            for h in range(2)
        ]
        line = lax.broadcasted_iota(jnp.int32, (16, LANES), 0)
        den = jnp.where((line & 1) == 0, den[0], den[1])
        high = den.astype(BF).astype(F32)
        m3[j, D0 : D0 + 16, :] = jnp.where(line < 2, high, jnp.where(line < 4, den - high, 0.0)).astype(BF)
        return carry

    lax.fori_loop(0, N, one_run, 0, unroll=8)
    @pl.when(c == 0)
    def _():
        for own, (sums, slices, carried) in enumerate(((TA0, SA0, CA0), (TB0, SB0, CB0))):
            which = head ^ own
            per_run, per_row = of_head(PER_RUN, which), of_head(PER_ROW, which)
            state = jnp.zeros((64, LANES), F32)
            for k in range(N):
                state = jnp.where(k < b, state * per_row + got2[k, sums : sums + 64, :].astype(F32), state)
            for j in range(N):
                m3[j, carried : carried + 64, :] = state.astype(BF)
                state = state * per_run + got1[j, slices : slices + 64, :].astype(F32)

    @pl.when(c == 1)
    def _():
        for j in range(N):
            for i in range(N):
                m3[j, CA0 + 16 * i : CA0 + 16 * i + 16, :] = got2[i, SPARE : SPARE + 16, :]


def output_kernel(got2, got3, sent, qrot, inner, keep, give, weight, mixed, state):
    _, _, _, c = places()
    rate = of_head(RATES, lax.axis_index("x") * 2 + c)
    @pl.when(c == 0)
    def _():
        for i in range(N):
            for k in range(N):
                at, start = (i * N + k) * 32, WW0 + 80 * k
                weight[at : at + 32, :LANES] = got2[i, start : start + 32, :]
                weight[at : at + 32, LANES : 2 * LANES] = got2[i, start + 32 : start + 64, :]
                weight[at : at + 16, 2 * LANES :] = got2[i, start + 64 : start + 80, :]
                at = (k * N + i) * 32
                weight[at + 16 : at + 32, 2 * LANES :] = sent[k, 16 * i : 16 * i + 16, :]
        for j in range(N):
            for half in range(2):
                piece = got3[j, CA0 + 32 * half : CA0 + 32 * half + 32, :]
                state[32 * j : 32 * j + 32, LANES * half : LANES * half + LANES] = piece

    @pl.when(c == 1)
    def _():
        for i in range(N):
            for k in range(N):
                at, start = (k * N + i) * 32, TA0 + 96 * k
                for h in range(3):
                    weight[at : at + 32, LANES * h : LANES * h + LANES] = got2[i, start + 32 * h : start + 32 * h + 32, :]
        for j in range(N):
            for half in range(2):
                piece = sent[j, 64 + 32 * half : 64 + 32 * half + 32, :]
                state[32 * j : 32 * j + 32, LANES * half : LANES * half + LANES] = piece

    num = got3[0, N0 : N0 + RUN, :].astype(F32)
    den = got3[0, D0 : D0 + 16, :].astype(F32)
    for j in range(1, N):
        num = num + got3[j, N0 : N0 + RUN, :].astype(F32)
        den = den + got3[j, D0 : D0 + 16, :].astype(F32)
    row = lax.broadcasted_iota(jnp.int32, (LANES, LANES), 0)
    col = lax.broadcasted_iota(jnp.int32, (LANES, LANES), 1)
    for h in range(2):
        line = den[h : h + 1, :] + den[h + 2 : h + 3, :]
        column = jnp.sum(jnp.where(row == col, line, 0.0), axis=1, keepdims=True)
        raw = num[LANES * h : LANES * h + LANES] / column
        raw = raw * lax.rsqrt(jnp.mean(raw * raw, axis=1, keepdims=True) + eps)
        mixed[LANES * h : LANES * h + LANES, RET:] = raw.astype(BF)
    steps = lax.broadcasted_iota(jnp.int32, (RUN, RET), 0)
    raw = inner[...] + dot(qrot[...], state[...]) * jnp.exp(-rate * (steps + 1).astype(F32))
    raw = raw * lax.rsqrt(jnp.mean(raw * raw, axis=1, keepdims=True) + eps)
    mixed[:, :RET] = raw.astype(BF)
    for side, target in ((c, keep), (1 - c, give)):
        rows = jnp.concatenate(
            [mixed[pl.ds(pl.multiple_of(64 * j + 32 * side, 32), 32), :] for j in range(4)], axis=0
        )
        for n in range(4):
            part = dot_nt(rows, weight[512 * n : 512 * n + 512, :])
            for j in range(4):
                target[j, :, 512 * n : 512 * n + 512] = part[32 * j : 32 * j + 32].astype(target.dtype)


def vmem(count):
    return [pl.BlockSpec(memory_space=pltpu.VMEM)] * count


def call(kernel, outs, scratch, args, flops, nbytes, name, limit, far=(), out_space=pltpu.VMEM):
    specs = vmem(len(args)) + [pl.BlockSpec(memory_space=pltpu.HBM)] * len(far)
    return pl.pallas_call(
        kernel,
        out_shape=outs,
        in_specs=specs,
        out_specs=[pl.BlockSpec(memory_space=out_space)] * len(outs),
        scratch_shapes=scratch,
        cost_estimate=pl.CostEstimate(flops=flops, bytes_accessed=nbytes, transcendentals=0),
        compiler_params=pltpu.CompilerParams(vmem_limit_bytes=limit << 20),
        name=name,
    )(*args, *far)


def struct(*shape, dtype=BF):
    return jax.ShapeDtypeStruct(shape, dtype)


def per_device(
    tokens, gain, w_ret_q, w_ret_k, w_ret_v, w_fox_q, w_fox_k, w_fox_v, fox_gates, w_out_ret, w_out_fox
):
    own = lax.all_to_all(jnp.broadcast_to(tokens[None], (4, 32, 2048)), "x", 0, 0, tiled=True)
    other = swapped(own)
    wt = jnp.concatenate([w_out_ret, w_out_fox], axis=0).reshape(3, LANES, 32).transpose(0, 2, 1)
    far = (
        own, gain.reshape(1, 2048), other, w_ret_k, w_ret_v, jnp.asarray(ROW_TURN), jnp.asarray(RUN_TURN),
        fox_gates.reshape(2, LANES), w_fox_q, wt,
    )
    made = [
        struct(N, R1, LANES), struct(N, 64, LANES), struct(RUN, 2048), struct(2, RUN, LANES, dtype=F32),
        struct(RUN, RET), struct(RUN, RET), struct(16, LANES),
    ]
    m1, states, *passed = call(
        project_kernel,
        made,
        [pltpu.VMEM(a.shape, a.dtype) for a in (*far, *made)]
        + [pltpu.SemaphoreType.DMA((len(far),)), pltpu.SemaphoreType.DMA((len(made),))],
        (), 700_000_000, 8_000_000, "project", 60, far, pltpu.HBM,
    )
    spare = swapped(states)
    m1 = lax.dynamic_update_slice(m1, spare, (0, SB0, 0))
    got1 = exchanged(m1, GROUPS_A)
    kvg, qrot, inner = call(
        rest_kernel,
        [struct(KG0 + 16, LANES), struct(RUN, RET), struct(RUN, RET, dtype=F32)],
        [], (*passed, w_ret_q, w_fox_k, w_fox_v), 700_000_000, 4_000_000, "rest", 20,
    )
    (m2,) = call(totals_kernel, [struct(N, R2, LANES)], [], (got1, kvg, spare), 1_000_000, 4_000_000, "totals", 16)
    got2 = exchanged(m2, GROUPS_B)
    (m3,) = call(
        attention_kernel,
        [struct(N, R3, LANES)],
        [pltpu.VMEM((N, RUN, 2 * LANES), BF), pltpu.VMEM((N, RUN, 2 * LANES), BF)],
        (got1, got2), 4_300_000_000, 4_000_000, "attention", 24,
    )
    got3 = exchanged(m3, GROUPS_A)
    sent = swapped(got3[:, CA0 : CA0 + 128, :])
    keep, give = call(
        output_kernel,
        [struct(4, 32, 2048, dtype=F32), struct(4, 32, 2048)],
        [pltpu.VMEM((2048, 384), BF), pltpu.VMEM((RUN, 384), BF), pltpu.VMEM((RET, RET), BF)],
        (got2, got3, sent, qrot, inner), 400_000_000, 4_000_000, "output", 20,
    )
    pair = (keep + swapped(give).astype(F32)).astype(BF)
    return jnp.sum(lax.all_to_all(pair, "x", 0, 0, tiled=True).astype(F32), axis=0).astype(BF)


def solution(mesh):
    split = Mesh(mesh.devices.reshape(N, N, 4, 2), ALL)
    return jax.shard_map(
        per_device,
        mesh=split,
        in_specs=(
            P(ALL, None),
            P(),
            P(None, TP),
            P(None, TP),
            P(None, TP),
            P(None, TP),
            P(None, TP),
            P(None, TP),
            P(SP, TP),
            P(TP, SP),
            P(TP, SP),
        ),
        out_specs=P(ALL, None),
        check_vma=False,
    )
```

```python
import functools
import math

import jax
import jax.numpy as jnp
import numpy as np
from jax import lax
from jax.experimental import pallas as pl
from jax.experimental.pallas import tpu as pltpu
from jax.sharding import Mesh
from jax.sharding import PartitionSpec as P

N = 8
RUN = 256
LANES = 128
RET = 256
FOX = 128
eps = 1e-06
ALL = ("z", "y", "x", "c")
SP = ("z", "y")
TP = ("x", "c")

Q0, QG0, SA0, SB0, W0, R1 = 0, 256, 272, 336, 400, 480
K0, V0, KG0, TA0, TB0, WW0, R2 = 0, 256, 512, 528, 592, 656, 1312
N0, D0, CA0, CB0, R3 = 0, 256, 272, 336, 400
SPARE = 1296

HEADS = np.arange(8, dtype=np.float64)
RATES = np.where(HEADS < 4, 1.0 / (32.0 + 16.0 * HEADS), np.exp2(-(HEADS - 4)) / 16384.0)
PER_RUN = np.exp(-RATES * RUN)
PER_ROW = np.exp(-RATES * RUN * N)
INVERSE = 10000.0 ** (-np.arange(LANES, dtype=np.float64) / LANES)
ROW_ANGLE = np.arange(RUN, dtype=np.float64)[:, None] * INVERSE
RUN_ANGLE = (RUN * np.arange(64, dtype=np.float64))[:, None] * INVERSE
ROW_TURN = np.stack([np.cos(ROW_ANGLE), np.sin(ROW_ANGLE)]).astype(np.float32)
RUN_TURN = np.stack([np.cos(RUN_ANGLE), np.sin(RUN_ANGLE)]).astype(np.float32)

BF = jnp.bfloat16
F32 = jnp.float32


def device_id(z, y, x, c):
    return ((z * N + y) * 4 + x) * 2 + c


Y_GROUPS = [[[device_id(z, y, x, c) for y in range(N)] for z in range(N) for x in range(4)] for c in (0, 1)]
Z_GROUPS = [[[device_id(z, y, x, c) for z in range(N)] for y in range(N) for x in range(4)] for c in (0, 1)]
GROUPS_A = Y_GROUPS[0] + Z_GROUPS[1]
GROUPS_B = Z_GROUPS[0] + Y_GROUPS[1]


def exchanged(message, groups):
    return lax.all_to_all(message, ALL, 0, 0, axis_index_groups=groups, tiled=True)


def swapped(array):
    return lax.ppermute(array, "c", [(0, 1), (1, 0)])


def places():
    z, y, c = lax.axis_index("z"), lax.axis_index("y"), lax.axis_index("c")
    first = c == 0
    return z * N + y, jnp.where(first, y, z), jnp.where(first, z, y), c


def of_head(table, head):
    value = jnp.float32(table[0])
    for h in range(1, 8):
        value = jnp.where(head == h, jnp.float32(table[h]), value)
    return value


def dot_nt(left, right):
    return lax.dot_general(left, right, (((1,), (1,)), ((), ())), preferred_element_type=F32)


def dot_tn(left, right):
    return lax.dot_general(left, right, (((0,), (0,)), ((), ())), preferred_element_type=F32)


def dot(left, right):
    return jnp.dot(left, right, preferred_element_type=F32)


def turned(values, cosine, sine, scale):
    first, second = values[:, :LANES], values[:, LANES:]
    return jnp.concatenate(
        [(first * cosine - second * sine) * scale, (first * sine + second * cosine) * scale], axis=1
    )


def project_kernel(*refs):
    far, outs = refs[:10], refs[10:17]
    near, made = refs[17:27], refs[27:34]
    in_sems, out_sems = refs[34:]
    copies = [pltpu.make_async_copy(src, dst, in_sems.at[k]) for k, (src, dst) in enumerate(zip(far, near))]
    for copy in copies:
        copy.start()
    own, gain, other, wrk, wrv, row_turn, run_turn, gates, wfq, wt = near
    m1, states, xs, turn, rkeys, rvalues, kgates = made
    stores = [pltpu.make_async_copy(src, dst, out_sems.at[k]) for k, (src, dst) in enumerate(zip(made, outs))]
    place, _, _, c = places()
    rate = of_head(RATES, lax.axis_index("x") * 2 + c)
    copies[0].wait()
    copies[1].wait()
    for part, side in ((own, c), (other, 1 - c)):
        if part is other:
            copies[2].wait()
        for j in range(4):
            x = part[j].astype(F32)
            scaled = x * lax.rsqrt(jnp.mean(x * x, axis=1, keepdims=True) + eps) * gain[...]
            xs[pl.ds(pl.multiple_of(64 * j + 32 * side, 32), 32), :] = scaled.astype(BF)
    stores[2].start()
    x = xs[...]
    for copy in copies[3:7]:
        copy.wait()
    cos_run = run_turn[0, pl.ds(place, 1), :]
    sin_run = run_turn[1, pl.ds(place, 1), :]
    cosine = row_turn[0] * cos_run - row_turn[1] * sin_run
    sine = row_turn[1] * cos_run + row_turn[0] * sin_run
    turn[0] = cosine
    turn[1] = sine
    stores[3].start()
    rk = turned(dot(x, wrk[...]).astype(BF).astype(F32), cosine, sine, RET**-0.5).astype(BF)
    rv = dot(x, wrv[...]).astype(BF)
    rkeys[...] = rk
    rvalues[...] = rv
    stores[4].start()
    stores[5].start()
    row = lax.broadcasted_iota(jnp.int32, (RUN, RET), 0)
    col = lax.broadcasted_iota(jnp.int32, (RUN, RET), 1)
    kd = (rk.astype(F32) * jnp.exp(-rate * (RUN - 1 - row).astype(F32))).astype(BF)
    state = dot_tn(kd, rv).astype(BF)
    for j in range(N):
        for half in range(2):
            piece = state[32 * j : 32 * j + 32, LANES * half : LANES * half + LANES]
            states[j, 32 * half : 32 * half + 32, :] = piece
    for copy in copies[7:10]:
        copy.wait()

    @pl.when(c == 0)
    def _():
        for j in range(N):
            m1[j, SA0 : SA0 + 64, :] = states[j]
            m1[j, W0 : W0 + 32, :] = wt[0]
            m1[j, W0 + 32 : W0 + 64, :] = wt[1]
            m1[j, W0 + 64 : W0 + 80, :] = wt[2, 0:16, :]
        states[0, 0:16, :] = wt[2, 16:32, :]

    @pl.when(c == 1)
    def _():
        for j in range(N):
            m1[j, SA0 : SA0 + 32, :] = wt[0]
            m1[j, SA0 + 32 : SA0 + 64, :] = wt[1]
            m1[j, W0 : W0 + 32, :] = wt[2]
            m1[j, W0 + 32 : W0 + 80, :] = jnp.zeros((48, LANES), BF)

    stores[1].start()
    fq = dot(x, wfq[...]).astype(BF)
    line = lax.broadcasted_iota(jnp.int32, (16, LANES), 0)
    gate = jnp.where(line < 8, gates[0:1, :], gates[1:2, :]) * (FOX**0.5)
    high = gate.astype(BF).astype(F32)
    middle = (gate - high).astype(BF).astype(F32)
    low = gate - high - middle
    slot = line & 7
    third = jnp.where(slot == 0, high, jnp.where(slot == 1, middle, low))
    of_query = jnp.where(slot < 3, third, jnp.where(slot < 6, 1.0, 0.0)).astype(BF)
    third = jnp.where(slot == 3, high, jnp.where(slot == 4, middle, low))
    of_key = jnp.where(slot < 3, 1.0, jnp.where(slot < 6, -third, 0.0)).astype(BF)
    for j in range(N):
        m1[j, Q0 : Q0 + RUN, :] = fq
        m1[j, QG0 : QG0 + 16, :] = of_query
        m1[j, SB0 : SB0 + 64, :] = jnp.zeros((64, LANES), BF)
    stores[0].start()
    kgates[...] = of_key
    stores[6].start()
    for store in stores:
        store.wait()


def rest_kernel(xs, turn, rkeys, rvalues, kgates, wrq, wfk, wfv, kvg, qrot, inner):
    rate = of_head(RATES, lax.axis_index("x") * 2 + lax.axis_index("c"))
    x = xs[...]
    kvg[KG0 : KG0 + 16, :] = kgates[...]
    kvg[K0 : K0 + RUN, :] = dot(x, wfk[...]).astype(BF)
    kvg[V0 : V0 + RUN, :] = dot(x, wfv[...]).astype(BF)
    rq = turned(dot(x, wrq[...]).astype(BF).astype(F32), turn[0], turn[1], 1.0).astype(BF)
    qrot[...] = rq
    row = lax.broadcasted_iota(jnp.int32, (RUN, RET), 0)
    spread = row - lax.broadcasted_iota(jnp.int32, (RUN, RET), 1)
    within = jnp.where(spread >= 0, jnp.exp(-rate * jnp.maximum(spread, 0).astype(F32)), 0.0)
    inner[...] = dot((dot_nt(rq, rkeys[...]) * within).astype(BF), rvalues[...])


def totals_kernel(got1, kvg, spare, m2):
    c = lax.axis_index("c")
    head = lax.axis_index("x") * 2 + c
    for j in range(N):
        m2[j, 0 : KG0 + 16, :] = kvg[...]

    @pl.when(c == 0)
    def _():
        sums = []
        for start, which in ((SA0, head), (SB0, head ^ 1)):
            decay = of_head(PER_RUN, which)
            total = got1[0, start : start + 64, :].astype(F32)
            for j in range(1, N):
                total = total * decay + got1[j, start : start + 64, :].astype(F32)
            sums.append(total.astype(BF))
        for j in range(N):
            m2[j, TA0 : TA0 + 64, :] = sums[0]
            m2[j, TB0 : TB0 + 64, :] = sums[1]
            for k in range(N):
                m2[j, WW0 + 80 * k : WW0 + 80 * k + 80, :] = got1[k, W0 : W0 + 80, :]
            m2[j, SPARE : SPARE + 16, :] = jnp.zeros((16, LANES), BF)

    @pl.when(c == 1)
    def _():
        for j in range(N):
            for k in range(N):
                m2[j, TA0 + 96 * k : TA0 + 96 * k + 64, :] = got1[k, SA0 : SA0 + 64, :]
                m2[j, TA0 + 96 * k + 64 : TA0 + 96 * k + 96, :] = got1[k, W0 : W0 + 32, :]
            m2[j, SPARE : SPARE + 16, :] = spare[0, 0:16, :]


def as_columns(rows, eye):
    lines = rows.astype(F32)
    wide = jnp.concatenate([lines[0:8], lines[8:16]], axis=1)
    wide = jnp.concatenate([wide, jnp.zeros((LANES - 8, RUN), F32)], axis=0).astype(BF)
    return dot_nt(eye, wide).astype(BF)


def attention_kernel(got1, got2, m3, keys, values):
    _, a, b, c = places()
    head = lax.axis_index("x") * 2 + c
    row = lax.broadcasted_iota(jnp.int32, (RUN, RUN), 0)
    col = lax.broadcasted_iota(jnp.int32, (RUN, RUN), 1)
    eye = jnp.where(row == col, 1.0, 0.0).astype(BF)
    diagonal = (row == col)[:LANES, :LANES]
    ahead = col - row
    for i in range(N):
        keys[i, :, :LANES] = got2[i, K0 : K0 + RUN, :]
        keys[i, :, LANES:] = as_columns(got2[i, KG0 : KG0 + 16, :], eye)
        values[i, :, :LANES] = got2[i, V0 : V0 + RUN, :]
        values[i, :, LANES:] = jnp.ones((RUN, LANES), BF)

    def one_run(j, carry):
        query = jnp.concatenate(
            [got1[j, Q0 : Q0 + RUN, :], as_columns(got1[j, QG0 : QG0 + 16, :], eye)], axis=1
        )
        of_query = jnp.where(c == 0, b * N + j, j * N + b)
        weights = []
        for i in range(N):
            of_key = jnp.where(c == 0, i * N + a, a * N + i)
            score = dot_nt(query, keys[i]) * (FOX**-0.5 * math.log2(math.e))
            score = jnp.where(ahead <= (of_query - of_key) * RUN, score, -jnp.inf)
            weights.append(jnp.exp2(score).astype(BF))
        total = dot(jnp.concatenate(weights, axis=1), values[...].reshape(N * RUN, 2 * LANES))
        m3[j, N0 : N0 + RUN, :] = total[:, :LANES].astype(BF)
        den = [
            jnp.sum(jnp.where(diagonal, total[LANES * h : LANES * h + LANES, LANES:], 0.0), axis=0, keepdims=True)
            for h in range(2)
        ]
        line = lax.broadcasted_iota(jnp.int32, (16, LANES), 0)
        den = jnp.where((line & 1) == 0, den[0], den[1])
        high = den.astype(BF).astype(F32)
        m3[j, D0 : D0 + 16, :] = jnp.where(line < 2, high, jnp.where(line < 4, den - high, 0.0)).astype(BF)
        return carry

    lax.fori_loop(0, N, one_run, 0, unroll=8)
    @pl.when(c == 0)
    def _():
        for own, (sums, slices, carried) in enumerate(((TA0, SA0, CA0), (TB0, SB0, CB0))):
            which = head ^ own
            per_run, per_row = of_head(PER_RUN, which), of_head(PER_ROW, which)
            state = jnp.zeros((64, LANES), F32)
            for k in range(N):
                state = jnp.where(k < b, state * per_row + got2[k, sums : sums + 64, :].astype(F32), state)
            for j in range(N):
                m3[j, carried : carried + 64, :] = state.astype(BF)
                state = state * per_run + got1[j, slices : slices + 64, :].astype(F32)

    @pl.when(c == 1)
    def _():
        for j in range(N):
            for i in range(N):
                m3[j, CA0 + 16 * i : CA0 + 16 * i + 16, :] = got2[i, SPARE : SPARE + 16, :]


def output_kernel(got2, got3, sent, qrot, inner, give, weight, mixed, state):
    _, _, _, c = places()
    rate = of_head(RATES, lax.axis_index("x") * 2 + c)
    @pl.when(c == 0)
    def _():
        for i in range(N):
            for k in range(N):
                at, start = (i * N + k) * 32, WW0 + 80 * k
                weight[at : at + 32, :LANES] = got2[i, start : start + 32, :]
                weight[at : at + 32, LANES : 2 * LANES] = got2[i, start + 32 : start + 64, :]
                weight[at : at + 16, 2 * LANES :] = got2[i, start + 64 : start + 80, :]
                at = (k * N + i) * 32
                weight[at + 16 : at + 32, 2 * LANES :] = sent[k, 16 * i : 16 * i + 16, :]
        for j in range(N):
            for half in range(2):
                piece = got3[j, CA0 + 32 * half : CA0 + 32 * half + 32, :]
                state[32 * j : 32 * j + 32, LANES * half : LANES * half + LANES] = piece

    @pl.when(c == 1)
    def _():
        for i in range(N):
            for k in range(N):
                at, start = (k * N + i) * 32, TA0 + 96 * k
                for h in range(3):
                    weight[at : at + 32, LANES * h : LANES * h + LANES] = got2[i, start + 32 * h : start + 32 * h + 32, :]
        for j in range(N):
            for half in range(2):
                piece = sent[j, 64 + 32 * half : 64 + 32 * half + 32, :]
                state[32 * j : 32 * j + 32, LANES * half : LANES * half + LANES] = piece

    num = got3[0, N0 : N0 + RUN, :].astype(F32)
    den = got3[0, D0 : D0 + 16, :].astype(F32)
    for j in range(1, N):
        num = num + got3[j, N0 : N0 + RUN, :].astype(F32)
        den = den + got3[j, D0 : D0 + 16, :].astype(F32)
    row = lax.broadcasted_iota(jnp.int32, (LANES, LANES), 0)
    col = lax.broadcasted_iota(jnp.int32, (LANES, LANES), 1)
    for h in range(2):
        line = den[h : h + 1, :] + den[h + 2 : h + 3, :]
        column = jnp.sum(jnp.where(row == col, line, 0.0), axis=1, keepdims=True)
        raw = num[LANES * h : LANES * h + LANES] / column
        raw = raw * lax.rsqrt(jnp.mean(raw * raw, axis=1, keepdims=True) + eps)
        mixed[LANES * h : LANES * h + LANES, RET:] = raw.astype(BF)
    steps = lax.broadcasted_iota(jnp.int32, (RUN, RET), 0)
    raw = inner[...] + dot(qrot[...], state[...]) * jnp.exp(-rate * (steps + 1).astype(F32))
    raw = raw * lax.rsqrt(jnp.mean(raw * raw, axis=1, keepdims=True) + eps)
    mixed[:, :RET] = raw.astype(BF)
    half_product(mixed, weight, 1 - c, give)


def half_product(mixed, weight, side, target):
    rows = jnp.concatenate(
        [mixed[pl.ds(pl.multiple_of(64 * j + 32 * side, 32), 32), :] for j in range(4)], axis=0
    )
    for n in range(4):
        part = dot_nt(rows, weight[512 * n : 512 * n + 512, :])
        for j in range(4):
            target[j, :, 512 * n : 512 * n + 512] = part[32 * j : 32 * j + 32].astype(target.dtype)


def keep_kernel(mixed, weight, keep):
    half_product(mixed, weight, lax.axis_index("c"), keep)


def vmem(count):
    return [pl.BlockSpec(memory_space=pltpu.VMEM)] * count


def call(kernel, outs, scratch, args, flops, nbytes, name, limit, far=(), out_space=pltpu.VMEM):
    specs = vmem(len(args)) + [pl.BlockSpec(memory_space=pltpu.HBM)] * len(far)
    return pl.pallas_call(
        kernel,
        out_shape=outs,
        in_specs=specs,
        out_specs=[pl.BlockSpec(memory_space=out_space)] * len(outs),
        scratch_shapes=scratch,
        cost_estimate=pl.CostEstimate(flops=flops, bytes_accessed=nbytes, transcendentals=0),
        compiler_params=pltpu.CompilerParams(vmem_limit_bytes=limit << 20),
        name=name,
    )(*args, *far)


def struct(*shape, dtype=BF):
    return jax.ShapeDtypeStruct(shape, dtype)


def per_device(
    tokens, gain, w_ret_q, w_ret_k, w_ret_v, w_fox_q, w_fox_k, w_fox_v, fox_gates, w_out_ret, w_out_fox
):
    own = lax.all_to_all(jnp.broadcast_to(tokens[None], (4, 32, 2048)), "x", 0, 0, tiled=True)
    other = swapped(own)
    wt = jnp.concatenate([w_out_ret, w_out_fox], axis=0).reshape(3, LANES, 32).transpose(0, 2, 1)
    far = (
        own, gain.reshape(1, 2048), other, w_ret_k, w_ret_v, jnp.asarray(ROW_TURN), jnp.asarray(RUN_TURN),
        fox_gates.reshape(2, LANES), w_fox_q, wt,
    )
    made = [
        struct(N, R1, LANES), struct(N, 64, LANES), struct(RUN, 2048), struct(2, RUN, LANES, dtype=F32),
        struct(RUN, RET), struct(RUN, RET), struct(16, LANES),
    ]
    m1, states, *passed = call(
        project_kernel,
        made,
        [pltpu.VMEM(a.shape, a.dtype) for a in (*far, *made)]
        + [pltpu.SemaphoreType.DMA((len(far),)), pltpu.SemaphoreType.DMA((len(made),))],
        (), 700_000_000, 8_000_000, "project", 60, far, pltpu.HBM,
    )
    spare = swapped(states)
    m1 = lax.dynamic_update_slice(m1, spare, (0, SB0, 0))
    got1 = exchanged(m1, GROUPS_A)
    kvg, qrot, inner = call(
        rest_kernel,
        [struct(KG0 + 16, LANES), struct(RUN, RET), struct(RUN, RET, dtype=F32)],
        [], (*passed, w_ret_q, w_fox_k, w_fox_v), 700_000_000, 4_000_000, "rest", 20,
    )
    (m2,) = call(totals_kernel, [struct(N, R2, LANES)], [], (got1, kvg, spare), 1_000_000, 4_000_000, "totals", 16)
    got2 = exchanged(m2, GROUPS_B)
    (m3,) = call(
        attention_kernel,
        [struct(N, R3, LANES)],
        [pltpu.VMEM((N, RUN, 2 * LANES), BF), pltpu.VMEM((N, RUN, 2 * LANES), BF)],
        (got1, got2), 4_300_000_000, 4_000_000, "attention", 24,
    )
    got3 = exchanged(m3, GROUPS_A)
    sent = swapped(got3[:, CA0 : CA0 + 128, :])
    give, weight, mixed = call(
        output_kernel,
        [struct(4, 32, 2048), struct(2048, 384), struct(RUN, 384)],
        [pltpu.VMEM((RET, RET), BF)],
        (got2, got3, sent, qrot, inner), 300_000_000, 4_000_000, "output", 20,
    )
    given = swapped(give)
    (keep,) = call(
        keep_kernel, [struct(4, 32, 2048, dtype=F32)], [], (mixed, weight), 200_000_000, 3_000_000, "keep", 8,
    )
    pair = (keep + given.astype(F32)).astype(BF)
    return jnp.sum(lax.all_to_all(pair, "x", 0, 0, tiled=True).astype(F32), axis=0).astype(BF)


def solution(mesh):
    split = Mesh(mesh.devices.reshape(N, N, 4, 2), ALL)
    return jax.shard_map(
        per_device,
        mesh=split,
        in_specs=(
            P(ALL, None),
            P(),
            P(None, TP),
            P(None, TP),
            P(None, TP),
            P(None, TP),
            P(None, TP),
            P(None, TP),
            P(SP, TP),
            P(TP, SP),
            P(TP, SP),
        ),
        out_specs=P(ALL, None),
        check_vma=False,
    )
```
